32 devices in a mesh: sp: 8 (over z, x), tp: 4 (over y, core).
Axes of the slice: x: 2, y: 2, z: 4, core: 2. Of those that a mesh axis runs over, the one named last changes fastest.
Arguments:
- moe_in: bfloat16 [1536, 2048], P('sp', 'tp'), may hold values from -6 to 6
- cotangent: bfloat16 [1536, 2048], P('sp', 'tp'), may hold values from -6 to 6
- routes: int32 [1536, 2], P('sp'), may hold values from 0 to 7, all different within a row; in each aligned block of 192 rows (0 to 191, 192 to 383, ...) at most 60 rows name the same one
- route_weight: float32 [1536, 2], P('sp'), may hold values from 0.2 to 1
- w_gate: bfloat16 [8, 3584, 2048], P('sp', 'tp'), may hold values from -0.125 to 0.125
- w_up: bfloat16 [8, 3584, 2048], P('sp', 'tp'), may hold values from -0.125 to 0.125
- w_down: bfloat16 [8, 3584, 2048], P('sp', 'tp'), may hold values from -0.09375 to 0.09375
- conv_pre: bfloat16 [1536, 2048], P('sp', 'tp'), may hold values from -6 to 6
- norm_mean: float32 [1536], P('sp'), may hold values from -3 to 3
- norm_rstd: float32 [1536], P('sp'), may hold values from 0.5 to 2
- ln_gain: float32 [2048], P('tp'), may hold values from 0.1 to 1.9
- ln_shift: float32 [2048], P('tp'), may hold values from -3 to 3
- taps: float32 [31, 2048], P(None, 'tp'), may hold values from -1 to 1
- w_proj: bfloat16 [2048, 2048], P('sp', 'tp'), may hold values from -0.125 to 0.125
Outputs:
- grad_up: bfloat16 [8, 3584, 2048], P('sp', 'tp')
- grad_down: bfloat16 [8, 3584, 2048], P('sp', 'tp')
- grad_stream: bfloat16 [1536, 2048], P('sp', 'tp')
- grad_proj: float32 [2048, 2048], P('sp', 'tp')
- grad_conv: bfloat16 [1536, 2048], P('sp', 'tp')
The draws below stay inside these ranges and needn't reach their ends.
Inputs may be any that keep to these rules, and one draw needn't show every extreme that they name: `routes`: each token names 2 different experts. Among the tokens of one index of sp no expert is named more than 60 times, a bound that some block reaches.
All inputs are finite; a program needn't handle non-finite values.
Results may differ from the reference program's by a relative error of at most 0.02.
Values may be sent and summed in bfloat16 or wider, within the bound.
A program may use at most 64 MiB of HBM per device.

```python
import math
import jax
import jax.numpy as jnp
import numpy as np
from jax import lax

D = 2048
FF_E = 3584
KW = 31
TOP = 2
TOK_DEV = 192
EXPERTS = 8
CAP = 60
TOKENS = 1536
N_SP = 8
N_TP = 4


def raised(drawn, key, source, target, shards_of, factor):
    owner, partner = [(jnp.arange(drawn.shape[dim]) // (drawn.shape[dim] // shards_of)).reshape([-1 if axis == dim else 1 for axis in range(drawn.ndim)]) for dim in (source, target)]
    chosen = jax.random.permutation(key, shards_of)[partner]
    strong = (owner == chosen) | (owner == (partner + shards_of // 2) % shards_of)
    return jnp.where(strong, factor * drawn, drawn)


def level_of(stream_key, shape, shards, low, top_value):
    level, own = 1.0, jax.random.fold_in(stream_key, 6)
    for position, shards_of in shards:
        heights = jnp.exp(jax.random.uniform(jax.random.fold_in(own, position), (shards_of,), jnp.float32, low / len(shards), top_value / len(shards)))
        level = level * jnp.repeat(heights, shape[position] // shards_of).reshape([-1 if axis == position else 1 for axis in range(len(shape))])
    return level


def routed_block(stream_key, own, number, rows, count, top, bound, skew):
    sequence = jax.random.permutation(stream_key, count)
    crowded, common = load_shares(count, rows * top, bound, skew, True), load_shares(count, rows * top, bound, skew, False)
    places = jnp.arange(count)

    def named(lengths, turn):
        used = int((lengths > 0).sum())
        fixed = max(1, used // 4)
        passed = fixed + (places - fixed + turn * (used - fixed)) % max(1, count - fixed)
        return jnp.zeros((count,), jnp.int32).at[sequence[jnp.where(places < fixed, places, passed)]].set(jnp.asarray(lengths, jnp.int32))

    lengths = jnp.where(number % 4 == 0, named(crowded, number // 4), named(common, number - number // 4 - 1))
    mixed = jax.random.permutation(jax.random.fold_in(own, 3), count)
    giver, sink = mixed[0:count // 2 * 2:2], mixed[1:count // 2 * 2:2]
    slack = jnp.minimum(lengths[giver] - 1, bound - lengths[sink]) // 2
    slack = jnp.where((giver == sequence[0]) | (sink == sequence[0]) | (lengths[sink] == 0), 0, jnp.maximum(slack, 0))
    passed = jax.random.randint(jax.random.fold_in(own, 4), (count // 2,), 0, 1 << 20) % (slack + 1)
    lengths = lengths.at[giver].add(-passed).at[sink].add(passed)
    members = jnp.searchsorted(jnp.cumsum(lengths), jnp.arange(rows * top), side="right").astype(jnp.int32)
    grid = members.reshape(top, rows).T
    grid = grid[jax.random.permutation(jax.random.fold_in(own, 1), rows)]
    turn = jax.random.randint(jax.random.fold_in(own, 2), (rows, 1), 0, top)
    return jnp.take_along_axis(grid, (jnp.arange(top)[None, :] + turn) % top, axis=1)


def load_shares(amount, total, limit, skew, full):
    weights = [(1 << 20) // math.isqrt(rank ** skew) + 1 for rank in range(1, amount + 1)]
    largest = limit if full else min(limit, max(-(-total // amount), total * weights[0] // sum(weights)))
    least = 1 if total - largest >= amount - 1 else 0
    given, spare = [largest] + [least] * (amount - 1), total - largest - least * (amount - 1)
    while spare > 0:
        free = [i for i in range(1, amount) if given[i] < largest] or [i for i in range(1, amount) if given[i] < limit]
        whole, left = sum([weights[i] for i in free]), spare
        for i in free:
            addition = min(limit - given[i], max(1, left * weights[i] // whole), spare)
            given[i] = given[i] + addition
            spare = spare - addition
    return np.array(given)


def normal_values(rng, shape, spread, most, shards=(), held_as=jnp.bfloat16):
    loudness = level_of(rng, shape, shards, -0.22, 0.18) if shards else 1.0
    entries = jax.random.normal(rng, shape, jnp.float32) * spread * loudness
    return jnp.minimum(jnp.maximum(entries, -most), most).astype(held_as)


def heavy_noise(stream_key, shape, deviation, bound, split, heavy, kind=jnp.bfloat16):
    entries = deviation * jax.random.normal(stream_key, shape, jnp.float32)
    if split:
        entries = entries * level_of(stream_key, shape, split, -0.22, 0.18)
    return jnp.clip(raised(entries, jax.random.fold_in(stream_key, 3), *heavy), -bound, bound).astype(kind)


def setup_inputs(seed: int = 0) -> dict:
    key_of = jax.random.split(jax.random.key(seed), 15)
    moe_in = normal_values(key_of[0], (TOKENS, D), 1.0, 6.0, ((0, 8), (1, 4)))
    cotangent = heavy_noise(key_of[1], (TOKENS, D), 1.0, 6.0, ((0, 8), (1, 4)), (0, 1, 8, 2.0))
    routes_keys = jax.random.split(jax.random.fold_in(key_of[2], 1), TOKENS // TOK_DEV)
    routes_turns = jax.random.permutation(jax.random.fold_in(key_of[2], 3), TOKENS // TOK_DEV)
    routes = jax.vmap(lambda own, number: routed_block(jax.random.fold_in(key_of[2], 2), own, number, TOK_DEV, EXPERTS, TOP, CAP, 2))(routes_keys, routes_turns).reshape((TOKENS, TOP))
    route_weight = jnp.clip(0.2 + 0.8 * jax.random.uniform(key_of[3], (TOKENS, TOP), jnp.float32) ** level_of(key_of[3], (TOKENS, TOP), ((0, 8),), -0.2, 0.2), 0.2, 1.0)
    w_gate = normal_values(key_of[4], (EXPERTS, FF_E, D), D ** -0.5, 0.125, ((0, 8), (1, 4)))
    w_up = normal_values(key_of[5], (EXPERTS, FF_E, D), D ** -0.5, 0.125, ((0, 8), (1, 4)))
    w_down = normal_values(key_of[6], (EXPERTS, FF_E, D), FF_E ** -0.5, 0.09375, ((0, 8), (1, 4)))
    conv_pre = normal_values(key_of[7], (TOKENS, D), 1.0, 6.0, ((0, 8), (1, 4)))
    norm_mean = normal_values(key_of[8], (TOKENS,), 0.5, 3.0, ((0, 8),), jnp.float32)
    norm_rstd = jnp.clip(jnp.exp(math.log(2.0) - 1.3862944 * jax.random.uniform(key_of[9], (TOKENS,), jnp.float32) ** level_of(key_of[9], (TOKENS,), ((0, 8),), -0.2, 0.2)), 0.5, 2.0)
    ln_gain = jnp.clip(1.0 + 0.18 * jax.random.normal(key_of[10], (D,), jnp.float32), 0.1, 1.9)
    ln_shift = normal_values(key_of[11], (D,), 0.5, 3.0, ((0, 4),), jnp.float32)
    taps = normal_values(key_of[12], (KW, D), KW ** -0.5, 1.0, ((1, 4),), jnp.float32)
    w_proj = normal_values(key_of[13], (D, D), D ** -0.5, 0.125, ((0, 8), (1, 4)))
    return {"moe_in": moe_in, "cotangent": cotangent, "routes": routes, "route_weight": route_weight, "w_gate": w_gate, "w_up": w_up, "w_down": w_down, "conv_pre": conv_pre, "norm_mean": norm_mean, "norm_rstd": norm_rstd, "ln_gain": ln_gain, "ln_shift": ln_shift, "taps": taps, "w_proj": w_proj}


def silu_slope(pre_value, sigmoid_value):
    return sigmoid_value * (1.0 + pre_value * (1.0 - sigmoid_value))


def expert_backward(packed):
    expert_rows, routed_rows, gate_weight, up_weight, down_weight = packed
    gate_pre = lax.dot_general(expert_rows, gate_weight, (((1,), (1,)), ((), ())), preferred_element_type=jnp.float32)
    up_pre = lax.dot_general(expert_rows, up_weight, (((1,), (1,)), ((), ())), preferred_element_type=jnp.float32)
    gate_sigmoid = jax.nn.sigmoid(gate_pre)
    gate_active = gate_pre * gate_sigmoid
    hidden = (gate_active * up_pre).astype(jnp.bfloat16)
    hidden_grad = lax.dot_general(routed_rows, down_weight, (((1,), (1,)), ((), ())), preferred_element_type=jnp.float32)
    grad_down = lax.dot_general(hidden, routed_rows, (((0,), (0,)), ((), ())), preferred_element_type=jnp.float32).astype(jnp.bfloat16)
    gate_grad = (hidden_grad * up_pre * silu_slope(gate_pre, gate_sigmoid)).astype(jnp.bfloat16)
    up_grad = (hidden_grad * gate_active).astype(jnp.bfloat16)
    grad_up = lax.dot_general(up_grad, expert_rows, (((0,), (0,)), ((), ())), preferred_element_type=jnp.float32).astype(jnp.bfloat16)
    row_count = expert_rows.shape[0]
    block_width = gate_weight.shape[0] // N_TP
    gate_blocks = gate_grad.astype(jnp.float32).reshape(row_count, N_TP, block_width)
    up_blocks = up_grad.astype(jnp.float32).reshape(row_count, N_TP, block_width)
    gate_wblocks = gate_weight.astype(jnp.float32).reshape(N_TP, block_width, D)
    up_wblocks = up_weight.astype(jnp.float32).reshape(N_TP, block_width, D)
    partial_rows = jnp.einsum("rbf,bfd->rbd", gate_blocks, gate_wblocks) + jnp.einsum("rbf,bfd->rbd", up_blocks, up_wblocks)
    partial_low = lax.optimization_barrier(partial_rows.astype(jnp.bfloat16))
    pair_grad = jnp.sum(partial_low.astype(jnp.float32), axis=1).astype(jnp.bfloat16)
    return grad_up, grad_down, pair_grad


def reference(moe_in, cotangent, routes, route_weight, w_gate, w_up, w_down, conv_pre, norm_mean, norm_rstd, ln_gain, ln_shift, taps, w_proj):
    per_expert = N_SP * CAP
    route_count = TOP * TOKENS
    route_ids = routes.reshape(N_SP, TOP * TOK_DEV)
    onehot = (route_ids[:, :, None] == jnp.arange(EXPERTS, dtype=jnp.int32)[None, None, :]).astype(jnp.int32)
    earlier = jnp.cumsum(onehot, axis=1) - onehot
    slot_ids = jnp.sum(earlier * onehot, axis=2)
    sources = jnp.arange(N_SP, dtype=jnp.int32)[:, None]
    targets = (route_ids * per_expert + sources * CAP + slot_ids).reshape(-1).astype(jnp.int32)
    table = jnp.full((EXPERTS * per_expert,), route_count, jnp.int32).at[targets].set(jnp.arange(route_count, dtype=jnp.int32))
    filled = (table < route_count)[:, None]
    route_of_slot = jnp.minimum(table, route_count - 1).astype(jnp.int32)
    routed_all = (route_weight[:, :, None] * cotangent.astype(jnp.float32)[:, None, :]).astype(jnp.bfloat16).reshape(route_count, D)
    zero_value = jnp.zeros((), jnp.bfloat16)
    expert_rows = jnp.where(filled, moe_in[route_of_slot // TOP], zero_value).reshape(EXPERTS, per_expert, D)
    routed_rows = jnp.where(filled, routed_all[route_of_slot], zero_value).reshape(EXPERTS, per_expert, D)
    grad_up, grad_down, pair_grad = lax.map(expert_backward, (expert_rows, routed_rows, w_gate, w_up, w_down))
    returned = pair_grad.reshape(EXPERTS * per_expert, D)[targets].astype(jnp.float32).reshape(TOKENS, TOP, D)
    grad_stream = (cotangent.astype(jnp.float32) + jnp.sum(returned, axis=1)).astype(jnp.bfloat16)
    normed = (conv_pre.astype(jnp.float32) - norm_mean[:, None]) * norm_rstd[:, None]
    pre_act = normed * ln_gain[None, :] + ln_shift[None, :]
    act_sigmoid = jax.nn.sigmoid(pre_act)
    activated = (pre_act * act_sigmoid).astype(jnp.bfloat16)
    act_grad = jnp.dot(grad_stream, w_proj, preferred_element_type=jnp.float32)
    grad_proj = lax.dot_general(grad_stream, activated, (((0,), (0,)), ((), ())), preferred_element_type=jnp.float32)
    normed_grad = act_grad * silu_slope(pre_act, act_sigmoid) * ln_gain[None, :]
    mean_first = jnp.mean(normed_grad, axis=1, keepdims=True)
    mean_second = jnp.mean(normed_grad * normed, axis=1, keepdims=True)
    conv_grad = norm_rstd[:, None] * (normed_grad - mean_first - normed * mean_second)
    padded = jnp.concatenate([conv_grad, jnp.zeros((KW - 1, D), jnp.float32)], axis=0)
    grad_conv = jnp.zeros((TOKENS, D), jnp.float32)
    for lag in range(KW):
        grad_conv = grad_conv + taps[lag][None, :] * padded[lag:lag + TOKENS]
    return grad_up, grad_down, grad_stream, grad_proj, grad_conv.astype(jnp.bfloat16)
```

```python
import functools

import jax
import jax.numpy as jnp
from jax import lax
from jax.experimental import pallas as pl
from jax.experimental.pallas import tpu as pltpu
from jax.sharding import PartitionSpec as P

MESH = pl.DeviceIdType.MESH
BF = jnp.bfloat16
F32 = jnp.float32


def flipped(index, step):
    value, bit = index, 1
    while bit <= step:
        if step & bit:
            value = value + bit * (1 - 2 * lax.rem(lax.div(index, bit), 2))
        bit *= 2
    return value


def tile(index, size):
    return pl.ds(pl.multiple_of(index * size, size), size)


def nn(left, right):
    return lax.dot_general(left, right, (((1,), (0,)), ((), ())), preferred_element_type=F32)


def nt(left, right):
    return lax.dot_general(left, right, (((1,), (1,)), ((), ())), preferred_element_type=F32)


def tn(left, right):
    return lax.dot_general(left, right, (((0,), (0,)), ((), ())), preferred_element_type=F32)


def layer_kernel(
    groups, lanes, across,
    moe_ref, cot_ref, cols_ref, lines_ref, conv_ref, gain_ref, shift_ref, taps_ref,
    gate_hbm, up_hbm, down_hbm, proj_hbm,
    gup_ref, gdown_ref, gstream_ref, gproj_ref, gconv_ref,
    gate_w, up_w, down_w, send, rows, work_a, work_b, work_c, hid, upg, gtg,
    part, half, summed, arrived, total, returned, chosen_back, gathered, mix, pieces,
    normed_s, slope_s, stat_out, stat_in, ext,
    load_sem, dsp_s, dsp_r, dy_s, dy_r, dc_s, dc_r, sw_s, sw_r, cy_s, cy_r, csp_s, csp_r,
    az_s, az_r, ax_s, ax_r, ty_s, ty_r, tc_s, tc_r, p_s, p_r, st_s, st_r, halo_s, halo_r,
):
    group, lane = (lax.axis_index("sp"), lax.axis_index("tp"))
    chips = lanes // 2
    depth = groups // across
    chip, core = (lax.div(lane, 2), lax.rem(lane, 2))
    level, column = (lax.div(group, across), lax.rem(group, across))
    tokens, width = moe_ref.shape
    channels = width * lanes
    hidden_units = gate_w.shape[0]
    slots = groups * (rows.shape[1] // groups)
    cap = slots // groups
    halves = 2
    per_half = groups // halves
    half_rows = slots // halves
    proj_rows = proj_hbm.shape[0]
    lag_count = taps_ref.shape[0]
    partner = (group, flipped(lane, 1))
    mine = tile(lane, width)

    barrier = pltpu.get_barrier_semaphore()
    for step in range(1, groups):
        pl.semaphore_signal(barrier, inc=1, device_id=(flipped(group, step), lane), device_id_type=MESH)
    for step in range(1, lanes):
        pl.semaphore_signal(barrier, inc=1, device_id=(group, flipped(lane, step)), device_id_type=MESH)

    def remote(source, target, sends, recvs, device):
        return pltpu.make_async_remote_copy(
            src_ref=source, dst_ref=target, send_sem=sends, recv_sem=recvs,
            device_id=device, device_id_type=MESH,
        )

    loads = [
        pltpu.make_async_copy(proj_hbm, gathered.at[group, pl.ds(0, proj_rows)], load_sem.at[0]),
        pltpu.make_async_copy(gate_hbm.at[0], gate_w, load_sem.at[1]),
        pltpu.make_async_copy(up_hbm.at[0], up_w, load_sem.at[2]),
        pltpu.make_async_copy(down_hbm.at[0], down_w, load_sem.at[3]),
    ]
    for copy in loads:
        copy.start()

    named_line = (lines_ref[0:1, :], lines_ref[1:2, :])
    weight_line = (lines_ref[2:3, :], lines_ref[3:4, :])
    named_col = (cols_ref[:, 2:3], cols_ref[:, 3:4])
    down_iota = lax.broadcasted_iota(jnp.int32, (tokens, tokens), 0)
    over_iota = lax.broadcasted_iota(jnp.int32, (tokens, tokens), 1)
    place = lax.broadcasted_iota(jnp.int32, (slots, tokens), 0).astype(F32)
    matches, slot_weight = ([], 0.0)
    for choice in range(2):
        same = jnp.where(named_col[0] == named_line[choice], 1.0, 0.0) + jnp.where(
            named_col[1] == named_line[choice], 1.0, 0.0
        )
        rank = jnp.sum(jnp.where(down_iota < over_iota, same, 0.0), axis=0, keepdims=True)
        match = place == named_line[choice] * float(cap) + rank
        matches.append(match)
        slot_weight = slot_weight + jnp.sum(
            jnp.where(match, weight_line[choice], 0.0), axis=1, keepdims=True
        )
    chosen = jnp.where(matches[0] | matches[1], 1.0, 0.0).astype(BF)
    send[0] = nn(chosen, moe_ref[...]).astype(BF)
    send[1] = (slot_weight * nn(chosen, cot_ref[...])).astype(BF)
    rows[0, 0:cap, mine] = send[0, 0:cap, :]
    rows[1, 0:cap, mine] = send[1, 0:cap, :]

    pl.semaphore_wait(barrier, groups + lanes - 2)

    def at_slot(step, lane_index):
        return rows.at[:, pl.ds(step * cap, cap), tile(lane_index, width)]

    outgoing = []

    def go(copy):
        copy.start()
        outgoing.append(copy)
        return copy

    dispatched, crossed, shared = ({}, {}, {})

    def forward(step):
        for turn in range(1, chips):
            crossed[step, turn] = go(remote(
                at_slot(step, lane), at_slot(step, lane), dy_s.at[step, turn], dy_r.at[step, turn],
                (group, flipped(lane, 2 * turn)),
            ))
        shared[step, 0] = go(remote(
            at_slot(step, lane), at_slot(step, lane), dc_s.at[step, 0], dc_r.at[step, 0], partner
        ))

    def relay(step):
        for turn in range(1, chips):
            crossed[step, turn].wait_recv()
            peer = flipped(lane, 2 * turn)
            shared[step, turn] = go(remote(
                at_slot(step, peer), at_slot(step, peer), dc_s.at[step, turn], dc_r.at[step, turn], partner
            ))

    forward(0)
    for step in range(1, groups):
        dispatched[step] = go(remote(
            send.at[:, pl.ds(step * cap, cap)], at_slot(step, lane),
            dsp_s.at[step], dsp_r.at[step], (flipped(group, step), lane),
        ))

    bounds = ((0, proj_rows), (proj_rows, tokens))

    def block(owner_level, owner_column, kind):
        return gathered.at[owner_level * across + owner_column, pl.ds(bounds[kind][0], bounds[kind][1])]

    def along(kind, way, hop):
        sign = 1 - 2 * way
        source_level = level - sign * hop
        here = block(source_level, column, kind)
        return remote(
            here, here, az_s.at[kind, way, hop], az_r.at[kind, way, hop],
            ((level + sign) * across + column, lane),
        )

    def along_valid(way, hop):
        if way == 0:
            return (level - hop >= 0) & (level + 1 < depth)
        return (level + hop < depth) & (level - 1 >= 0)

    def arrives_valid(way, hop):
        if way == 0:
            return level - 1 - hop >= 0
        return level + 1 + hop < depth

    def sideways(kind, event, owner_level):
        copies = []
        for turn in range(1, across):
            here = block(owner_level, column, kind)
            copies.append(remote(
                here, here, ax_s.at[kind, event, turn], ax_r.at[kind, event, turn],
                (level * across + flipped(column, turn), lane),
            ))
        return copies

    def gather_own(kind):
        for way in range(2):
            @pl.when(along_valid(way, 0))
            def _():
                along(kind, way, 0).start()
        for copy in sideways(kind, 0, level):
            copy.start()

    def gather_hop(kind, hop):
        for way in range(2):
            sign = 1 - 2 * way

            @pl.when(arrives_valid(way, hop))
            def _():
                along(kind, way, hop).wait_recv()
                if hop + 1 < depth - 1:
                    @pl.when(along_valid(way, hop + 1))
                    def _():
                        along(kind, way, hop + 1).start()
                for copy in sideways(kind, 1 + 2 * hop + way, level - sign * (hop + 1)):
                    copy.start()

    def gather_rest(kind):
        for copy in sideways(kind, 0, level):
            copy.wait()
        for hop in range(depth - 1):
            for way in range(2):
                sign = 1 - 2 * way

                @pl.when(along_valid(way, hop))
                def _():
                    along(kind, way, hop).wait_send()

                @pl.when(arrives_valid(way, hop))
                def _():
                    for copy in sideways(kind, 1 + 2 * hop + way, level - sign * (hop + 1)):
                        copy.wait()

    loads[0].wait()
    gather_own(0)

    normed = (conv_ref[...].astype(F32) - cols_ref[:, 0:1]) * cols_ref[:, 1:2]
    pre_act = normed * gain_ref[...] + shift_ref[...]
    act_sigmoid = jax.nn.sigmoid(pre_act)
    gathered[group, proj_rows : proj_rows + tokens, :] = (pre_act * act_sigmoid).astype(BF)
    normed_s[...] = normed
    slope_s[...] = act_sigmoid * (1.0 + pre_act * (1.0 - act_sigmoid)) * gain_ref[...]
    back_place = lax.broadcasted_iota(jnp.int32, (tokens, slots), 1).astype(F32)
    back = None
    for choice in range(2):
        same = jnp.where(named_line[0] == named_col[choice], 1.0, 0.0) + jnp.where(
            named_line[1] == named_col[choice], 1.0, 0.0
        )
        rank = jnp.sum(jnp.where(over_iota < down_iota, same, 0.0), axis=1, keepdims=True)
        match = back_place == named_col[choice] * float(cap) + rank
        back = match if back is None else back | match
    chosen_back[...] = jnp.where(back, 1.0, 0.0).astype(BF)

    def of_half(part_index):
        return slice(part_index * half_rows, (part_index + 1) * half_rows)

    def activate(part_index):
        here = of_half(part_index)
        step_rows = 64

        def body(index, carry):
            there = tile(index, step_rows)
            gate_pre, up_pre, hidden_grad = (work_a[there, :], work_b[there, :], work_c[there, :])
            gate_sigmoid = jax.nn.sigmoid(gate_pre)
            gate_active = gate_pre * gate_sigmoid
            hid[there, here] = (gate_active * up_pre).astype(BF)
            upg[there, here] = (hidden_grad * gate_active).astype(BF)
            gtg[there, here] = (
                hidden_grad * up_pre * (gate_sigmoid * (1.0 + gate_pre * (1.0 - gate_sigmoid)))
            ).astype(BF)
            return carry

        lax.fori_loop(0, hidden_units // step_rows, body, 0)

    def partial_columns(part_index, lane_index):
        here = of_half(part_index)
        there = tile(lane_index, width)
        value = tn(gtg[:, here], gate_w[:, there]) + tn(upg[:, here], up_w[:, there])
        part[here, there] = value.astype(BF)

    swaps, homeward, back_across = ({}, {}, {})

    def swap(part_index, turn):
        away = flipped(lane, 2 * turn + 1)
        here = pl.ds(part_index * half_rows, half_rows)
        swaps[part_index, turn] = go(remote(
            part.at[here, tile(away, width)], half.at[turn, here],
            sw_s.at[part_index, turn], sw_r.at[part_index, turn], partner,
        ))

    def partials(part_index):
        for turn in [*range(1, chips), 0]:
            partial_columns(part_index, flipped(lane, 2 * turn + 1))
            swap(part_index, turn)
            partial_columns(part_index, flipped(lane, 2 * turn))

    def chip_sums(part_index):
        for turn in range(1, chips):
            away = flipped(lane, 2 * turn)
            swaps[part_index, turn].wait_recv()
            for step in range(part_index * per_half, (part_index + 1) * per_half):
                here = slice(step * cap, (step + 1) * cap)
                summed[turn - 1, here, :] = (
                    part[here, tile(away, width)].astype(F32) + half[turn, here, :].astype(F32)
                ).astype(BF)
                back_across[step, turn] = go(remote(
                    summed.at[turn - 1, pl.ds(step * cap, cap)], arrived.at[turn - 1, pl.ds(step * cap, cap)],
                    cy_s.at[step, turn], cy_r.at[step, turn], (group, away),
                ))

    def send_home(part_index):
        swaps[part_index, 0].wait_recv()
        for step in range(part_index * per_half, (part_index + 1) * per_half):
            here = slice(step * cap, (step + 1) * cap)
            value = part[here, mine].astype(F32) + half[0, here, :].astype(F32)
            for turn in range(1, chips):
                back_across[step, turn].wait_recv()
                value = value + arrived[turn - 1, here, :].astype(F32)
            if step:
                total[here, :] = value.astype(BF)
                homeward[step] = go(remote(
                    total.at[pl.ds(step * cap, cap)], returned.at[pl.ds(step * cap, cap)],
                    csp_s.at[step], csp_r.at[step], (flipped(group, step), lane),
                ))
            else:
                returned[here, :] = value.astype(BF)

    for step in range(1, per_half):
        dispatched[step].wait_recv()
        forward(step)
        relay(step - 1)
    far = list(range(per_half, groups))
    quarter = max(1, len(far) // 4)
    for step in far[:quarter]:
        dispatched[step].wait_recv()
        forward(step)
    relay(per_half - 1)
    for step in range(per_half):
        for turn in range(chips):
            shared[step, turn].wait_recv()
    near = of_half(0)
    for copy in loads[1:]:
        copy.wait()
    work_a[...] = nt(gate_w[...], rows[0, near, :])
    for step in far[quarter : 2 * quarter]:
        dispatched[step].wait_recv()
        forward(step)
    work_b[...] = nt(up_w[...], rows[0, near, :])
    work_c[...] = nt(down_w[...], rows[1, near, :])
    for step in far[2 * quarter : 3 * quarter]:
        dispatched[step].wait_recv()
        forward(step)
    activate(0)
    for step in far[:quarter]:
        relay(step)
    partials(0)
    for step in far[3 * quarter :]:
        dispatched[step].wait_recv()
        forward(step)
    for step in far[quarter:]:
        relay(step)
    chip_sums(0)

    for step in far:
        for turn in range(chips):
            shared[step, turn].wait_recv()
    beyond = of_half(1)
    work_a[...] = nt(gate_w[...], rows[0, beyond, :])
    gather_hop(0, 0)
    work_b[...] = nt(up_w[...], rows[0, beyond, :])
    work_c[...] = nt(down_w[...], rows[1, beyond, :])
    activate(1)
    send_home(0)
    partials(1)
    chip_sums(1)
    for hop in range(1, depth - 1):
        gather_hop(0, hop)
    send_home(1)
    gather_own(1)

    span = min(channels, 512)

    def down_tile(index, carry):
        there = tile(index, span)
        gdown_ref[0, :, there] = nn(hid[...], rows[1, :, there]).astype(BF)
        return carry

    def up_tile(index, carry):
        there = tile(index, span)
        gup_ref[0, :, there] = nn(upg[...], rows[0, :, there]).astype(BF)
        return carry

    lax.fori_loop(0, channels // span, down_tile, 0)
    gather_hop(1, 0)
    lax.fori_loop(0, channels // span, up_tile, 0)

    for step in range(1, groups):
        homeward[step].wait_recv()
    picked = nn(chosen_back[...], returned[...])
    own_stream = (cot_ref[...].astype(F32) + picked).astype(BF)
    gstream_ref[...] = own_stream
    mix[:, mine] = own_stream
    tp_across = {}
    for turn in range(1, chips):
        tp_across[turn] = go(remote(
            mix.at[:, mine], mix.at[:, mine], ty_s.at[turn], ty_r.at[turn], (group, flipped(lane, 2 * turn))
        ))
    tp_shared = {0: go(remote(mix.at[:, mine], mix.at[:, mine], tc_s.at[0], tc_r.at[0], partner))}
    for turn in range(1, chips):
        tp_across[turn].wait_recv()
        theirs = tile(flipped(lane, 2 * turn), width)
        tp_shared[turn] = go(remote(
            mix.at[:, theirs], mix.at[:, theirs], tc_s.at[turn], tc_r.at[turn], partner
        ))
    gather_rest(0)
    for turn in range(chips):
        tp_shared[turn].wait_recv()
    for hop in range(1, depth - 1):
        gather_hop(1, hop)

    share = channels // groups
    piece_width = pieces.shape[2]

    def piece_of(owner):
        if share == piece_width:
            return tile(owner, share)
        return tile(lax.div(owner * share, piece_width), piece_width)

    travelling = {}
    for step in range(1, groups):
        owner = flipped(group, step)
        travelling[step] = go(remote(
            mix.at[:, piece_of(owner)], pieces.at[step], p_s.at[step], p_r.at[step], (owner, lane)
        ))

    whole_proj = gathered[:, 0:proj_rows, :].reshape(groups * proj_rows, width)
    normed_grad = nn(mix[...], whole_proj) * slope_s[...]
    weighted = normed_grad * normed_s[...]
    ones = jnp.ones((16, width), BF)

    def line_sum(value):
        high = value.astype(BF)
        low = (value - high.astype(F32)).astype(BF)
        return nt(ones, high) + nt(ones, low)

    line = lax.broadcasted_iota(jnp.int32, (16, tokens), 0)
    own_stat = jnp.where(line == 0, line_sum(normed_grad), line_sum(weighted))
    stat_out[...] = own_stat
    stats = []
    for step in range(1, lanes):
        stats.append(go(remote(
            stat_out, stat_in.at[step], st_s.at[step], st_r.at[step], (group, flipped(lane, step))
        )))
    all_stat = own_stat
    for step in range(1, lanes):
        stats[step - 1].wait_recv()
        all_stat = all_stat + stat_in[step]
    all_stat = all_stat * (1.0 / channels)
    high = all_stat.astype(BF)
    middle = (all_stat - high.astype(F32)).astype(BF)
    low = (all_stat - high.astype(F32) - middle.astype(F32)).astype(BF)
    pick = lax.broadcasted_iota(jnp.int32, (16, width), 0)

    def spread_line(number):
        chooser = jnp.where(pick == number, 1.0, 0.0).astype(BF)
        return tn(high, chooser) + tn(middle, chooser) + tn(low, chooser)

    ext[0:tokens, :] = cols_ref[:, 1:2] * (
        normed_grad - spread_line(0) - normed_s[...] * spread_line(1)
    )
    rim = ext.shape[0] - tokens

    def halo():
        return remote(
            ext.at[pl.ds(0, rim)], ext.at[pl.ds(tokens, rim)], halo_s, halo_r, (group - 1, lane)
        )

    @pl.when(group > 0)
    def _():
        halo().start()

    def piece_value(value):
        if share == piece_width:
            return value
        per = piece_width // share
        which = lax.rem(group, per)
        result = value[:, 0:share]
        for index in range(1, per):
            result = jnp.where(which == index, value[:, index * share : (index + 1) * share], result)
        return result

    for hop in range(depth - 1, depth - 1):
        gather_hop(1, hop)
    gather_rest(1)
    gproj = tn(piece_value(mix[:, piece_of(group)]), gathered[group, proj_rows : proj_rows + tokens, :])
    for step in range(1, groups):
        travelling[step].wait_recv()
        owner = flipped(group, step)
        gproj = gproj + tn(piece_value(pieces[step]), gathered[owner, proj_rows : proj_rows + tokens, :])
    gproj_ref[...] = gproj

    @pl.when(group < groups - 1)
    def _():
        halo().wait_recv()

    @pl.when(group == groups - 1)
    def _():
        ext[tokens : tokens + rim, :] = jnp.zeros((rim, width), F32)

    def conv_tile(index, carry):
        there = tile(index, 128)
        chunk = 64
        for start in range(0, tokens, chunk):
            value = jnp.zeros((chunk, 128), F32)
            for lag in range(lag_count):
                value = value + taps_ref[lag : lag + 1, there] * ext[start + lag : start + lag + chunk, there]
            gconv_ref[start : start + chunk, there] = value.astype(BF)
        return carry

    lax.fori_loop(0, width // 128, conv_tile, 0)

    @pl.when(group > 0)
    def _():
        halo().wait_send()

    for copy in outgoing:
        copy.wait_send()


def on_device(
    moe_in, cotangent, routes, route_weight, w_gate, w_up, w_down,
    conv_pre, norm_mean, norm_rstd, ln_gain, ln_shift, taps, w_proj,
):
    groups, lanes = (lax.axis_size("sp"), lax.axis_size("tp"))
    chips = lanes // 2
    across = 1 << (groups.bit_length() // 2 - 1)
    depth = groups // across
    group = lax.axis_index("sp")
    tokens, width = moe_in.shape
    channels = width * lanes
    hidden_units = w_gate.shape[1]
    cap = (5 * tokens // (2 * groups) + 15) // 16 * 16
    slots = groups * cap
    half_rows = slots // 2
    proj_rows = w_proj.shape[0]
    share = channels // groups
    piece_width = max(share, 128)
    rim = (taps.shape[0] - 1 + 7) // 8 * 8
    named = (routes ^ group).astype(F32)
    cols = jnp.concatenate([norm_mean[:, None], norm_rstd[:, None], named], axis=1)
    lines = jnp.concatenate([named.T, route_weight.T], axis=0)
    dma = pltpu.SemaphoreType.DMA
    vmem = pltpu.VMEM
    others = max(1, chips - 1)
    inside = pl.BlockSpec(memory_space=pltpu.VMEM)
    outside = pl.BlockSpec(memory_space=pl.ANY)
    return pl.pallas_call(
        functools.partial(layer_kernel, groups, lanes, across),
        out_shape=(
            jax.ShapeDtypeStruct(w_up.shape, BF),
            jax.ShapeDtypeStruct(w_down.shape, BF),
            jax.ShapeDtypeStruct((tokens, width), BF),
            jax.ShapeDtypeStruct((proj_rows, width), F32),
            jax.ShapeDtypeStruct((tokens, width), BF),
        ),
        in_specs=[inside] * 8 + [outside] * 4,
        out_specs=(inside,) * 5,
        scratch_shapes=[
            vmem((hidden_units, channels), BF), vmem((hidden_units, channels), BF), vmem((hidden_units, channels), BF),
            vmem((2, slots, width), BF), vmem((2, slots, channels), BF),
            vmem((hidden_units, half_rows), F32), vmem((hidden_units, half_rows), F32), vmem((hidden_units, half_rows), F32),
            vmem((hidden_units, slots), BF), vmem((hidden_units, slots), BF), vmem((hidden_units, slots), BF),
            vmem((slots, channels), BF), vmem((chips, slots, width), BF),
            vmem((others, slots, width), BF), vmem((others, slots, width), BF),
            vmem((slots, width), BF), vmem((slots, width), BF), vmem((tokens, slots), BF),
            vmem((groups, proj_rows + tokens, width), BF), vmem((tokens, channels), BF),
            vmem((groups, tokens, piece_width), BF),
            vmem((tokens, width), F32), vmem((tokens, width), F32),
            vmem((16, tokens), F32), vmem((lanes, 16, tokens), F32), vmem((tokens + rim, width), F32),
            dma((4,)), dma((groups,)), dma((groups,)),
            dma((groups, chips)), dma((groups, chips)), dma((groups, chips)), dma((groups, chips)),
            dma((2, chips)), dma((2, chips)), dma((groups, chips)), dma((groups, chips)),
            dma((groups,)), dma((groups,)),
            dma((2, 2, depth)), dma((2, 2, depth)), dma((2, 2 * depth, across)), dma((2, 2 * depth, across)),
            dma((chips,)), dma((chips,)), dma((chips,)), dma((chips,)),
            dma((groups,)), dma((groups,)), dma((lanes,)), dma((lanes,)), dma, dma,
        ],
        compiler_params=pltpu.CompilerParams(
            collective_id=1, has_side_effects=True, vmem_limit_bytes=60 * 1024 * 1024
        ),
    )(
        moe_in, cotangent, cols, lines, conv_pre, ln_gain[None, :], ln_shift[None, :], taps,
        w_gate, w_up, w_down, w_proj,
    )


def solution(mesh):
    placed = (
        P("sp", "tp"), P("sp", "tp"), P("sp", None), P("sp", None),
        P("sp", "tp", None), P("sp", "tp", None), P("sp", "tp", None),
        P("sp", "tp"), P("sp"), P("sp"), P("tp"), P("tp"), P(None, "tp"), P("sp", "tp"),
    )
    return jax.shard_map(
        on_device,
        mesh=mesh,
        in_specs=placed,
        out_specs=(
            P("sp", "tp", None), P("sp", "tp", None), P("sp", "tp"), P("sp", "tp"), P("sp", "tp"),
        ),
        check_vma=False,
    )
```

```python
import functools

import jax
import jax.numpy as jnp
from jax import lax
from jax.experimental import pallas as pl
from jax.experimental.pallas import tpu as pltpu
from jax.sharding import PartitionSpec as P

MESH = pl.DeviceIdType.MESH
BF = jnp.bfloat16
F32 = jnp.float32


def flipped(index, step):
    value, bit = index, 1
    while bit <= step:
        if step & bit:
            value = value + bit * (1 - 2 * lax.rem(lax.div(index, bit), 2))
        bit *= 2
    return value


def tile(index, size):
    return pl.ds(pl.multiple_of(index * size, size), size)


def nn(left, right):
    return lax.dot_general(left, right, (((1,), (0,)), ((), ())), preferred_element_type=F32)


def nt(left, right):
    return lax.dot_general(left, right, (((1,), (1,)), ((), ())), preferred_element_type=F32)


def tn(left, right):
    return lax.dot_general(left, right, (((0,), (0,)), ((), ())), preferred_element_type=F32)


def layer_kernel(
    groups, lanes, across,
    moe_ref, cot_ref, route_ref, weight_ref, mean_ref, rstd_ref, conv_ref, gain_ref, shift_ref, taps_ref,
    gate_hbm, up_hbm, down_hbm, proj_hbm,
    gup_ref, gdown_ref, gstream_ref, gproj_ref, gconv_ref,
    gate_w, up_w, down_w, send, rows, work_a, work_b, work_c, hid, upg, gtg,
    part, half, summed, arrived, total, returned, chosen_back, gathered, mix, pieces,
    lines_s, normed_s, slope_s, stat_out, stat_in, ext,
    load_sem, dsp_s, dsp_r, dy_s, dy_r, dc_s, dc_r, sw_s, sw_r, cy_s, cy_r, csp_s, csp_r,
    az_s, az_r, ax_s, ax_r, ty_s, ty_r, tc_s, tc_r, p_s, p_r, py_s, py_r, pc_s, pc_r, st_s, st_r, halo_s, halo_r,
):
    group, lane = (lax.axis_index("sp"), lax.axis_index("tp"))
    chips = lanes // 2
    depth = groups // across
    chip, core = (lax.div(lane, 2), lax.rem(lane, 2))
    level, column = (lax.div(group, across), lax.rem(group, across))
    tokens, width = moe_ref.shape
    channels = width * lanes
    hidden_units = gate_w.shape[0]
    slots = groups * (rows.shape[1] // groups)
    cap = slots // groups
    chunks = ((0, 3 * groups // 4), (3 * groups // 4, groups))
    proj_rows = proj_hbm.shape[0]
    lag_count = taps_ref.shape[0]
    partner = (group, flipped(lane, 1))
    mine = tile(lane, width)

    barrier = pltpu.get_barrier_semaphore()
    for step in range(1, groups):
        pl.semaphore_signal(barrier, inc=1, device_id=(flipped(group, step), lane), device_id_type=MESH)
    for step in range(1, lanes):
        pl.semaphore_signal(barrier, inc=1, device_id=(group, flipped(lane, step)), device_id_type=MESH)

    def remote(source, target, sends, recvs, device):
        return pltpu.make_async_remote_copy(
            src_ref=source, dst_ref=target, send_sem=sends, recv_sem=recvs,
            device_id=device, device_id_type=MESH,
        )

    loads = [
        pltpu.make_async_copy(proj_hbm, gathered.at[group, pl.ds(0, proj_rows)], load_sem.at[0]),
        pltpu.make_async_copy(gate_hbm.at[0], gate_w, load_sem.at[1]),
        pltpu.make_async_copy(up_hbm.at[0], up_w, load_sem.at[2]),
        pltpu.make_async_copy(down_hbm.at[0], down_w, load_sem.at[3]),
    ]
    for copy in loads:
        copy.start()

    lines_s[...] = jnp.zeros(lines_s.shape, F32)
    lines_s[0:2, 0:tokens] = (route_ref[...] ^ group).astype(F32)
    lines_s[2:3, 0:tokens] = mean_ref[...]
    lines_s[3:4, 0:tokens] = rstd_ref[...]
    named_line = (lines_s[0:1, 0:tokens], lines_s[1:2, 0:tokens])
    weight_line = (weight_ref[0:1, :], weight_ref[1:2, :])
    columns = lines_s[...].T
    named_col = (columns[0:tokens, 0:1], columns[0:tokens, 1:2])
    mean_col, rstd_col = (columns[0:tokens, 2:3], columns[0:tokens, 3:4])
    down_iota = lax.broadcasted_iota(jnp.int32, (tokens, tokens), 0)
    over_iota = lax.broadcasted_iota(jnp.int32, (tokens, tokens), 1)
    targets = []
    for choice in range(2):
        same = jnp.where(named_col[0] == named_line[choice], 1.0, 0.0) + jnp.where(
            named_col[1] == named_line[choice], 1.0, 0.0
        )
        rank = jnp.sum(jnp.where(down_iota < over_iota, same, 0.0), axis=0, keepdims=True)
        targets.append(named_line[choice] * float(cap) + rank)

    def fill(low, high):
        here = slice(low * cap, high * cap)
        count = (high - low) * cap
        place = lax.broadcasted_iota(jnp.int32, (count, tokens), 0).astype(F32) + float(low * cap)
        first, second = (place == targets[0], place == targets[1])
        slot_weight = jnp.sum(
            jnp.where(first, weight_line[0], 0.0) + jnp.where(second, weight_line[1], 0.0),
            axis=1, keepdims=True,
        )
        chosen = jnp.where(first | second, 1.0, 0.0).astype(BF)
        send[0, here, :] = nn(chosen, moe_ref[...]).astype(BF)
        send[1, here, :] = (slot_weight * nn(chosen, cot_ref[...])).astype(BF)

    fill(0, groups // 2)
    rows[0, 0:cap, mine] = send[0, 0:cap, :]
    rows[1, 0:cap, mine] = send[1, 0:cap, :]

    pl.semaphore_wait(barrier, groups + lanes - 2)

    def at_slot(step, lane_index):
        return rows.at[:, pl.ds(step * cap, cap), tile(lane_index, width)]

    outgoing = []

    def go(copy):
        copy.start()
        outgoing.append(copy)
        return copy

    dispatched, crossed, shared = ({}, {}, {})

    def forward(step):
        for turn in range(1, chips):
            crossed[step, turn] = go(remote(
                at_slot(step, lane), at_slot(step, lane), dy_s.at[step, turn], dy_r.at[step, turn],
                (group, flipped(lane, 2 * turn)),
            ))
        shared[step, 0] = go(remote(
            at_slot(step, lane), at_slot(step, lane), dc_s.at[step, 0], dc_r.at[step, 0], partner
        ))

    def relay(step):
        for turn in range(1, chips):
            crossed[step, turn].wait_recv()
            peer = flipped(lane, 2 * turn)
            shared[step, turn] = go(remote(
                at_slot(step, peer), at_slot(step, peer), dc_s.at[step, turn], dc_r.at[step, turn], partner
            ))

    def dispatch(step):
        dispatched[step] = go(remote(
            send.at[:, pl.ds(step * cap, cap)], at_slot(step, lane),
            dsp_s.at[step], dsp_r.at[step], (flipped(group, step), lane),
        ))

    forward(0)
    for step in range(1, groups // 2):
        dispatch(step)
    fill(groups // 2, groups)
    for step in range(groups // 2, groups):
        dispatch(step)

    bounds = ((0, proj_rows), (proj_rows, tokens))

    def block(owner_level, owner_column, kind):
        return gathered.at[owner_level * across + owner_column, pl.ds(bounds[kind][0], bounds[kind][1])]

    def along(kind, way, hop):
        sign = 1 - 2 * way
        source_level = level - sign * hop
        here = block(source_level, column, kind)
        return remote(
            here, here, az_s.at[kind, way, hop], az_r.at[kind, way, hop],
            ((level + sign) * across + column, lane),
        )

    def along_valid(way, hop):
        if way == 0:
            return (level - hop >= 0) & (level + 1 < depth)
        return (level + hop < depth) & (level - 1 >= 0)

    def arrives_valid(way, hop):
        if way == 0:
            return level - 1 - hop >= 0
        return level + 1 + hop < depth

    def sideways(kind, event, owner_level):
        copies = []
        for turn in range(1, across):
            here = block(owner_level, column, kind)
            copies.append(remote(
                here, here, ax_s.at[kind, event, turn], ax_r.at[kind, event, turn],
                (level * across + flipped(column, turn), lane),
            ))
        return copies

    def gather_along(kind):
        for way in range(2):
            @pl.when(along_valid(way, 0))
            def _():
                along(kind, way, 0).start()

    def gather_sideways(kind):
        for copy in sideways(kind, 0, level):
            copy.start()

    def gather_hop(kind, hop):
        for way in range(2):
            sign = 1 - 2 * way

            @pl.when(arrives_valid(way, hop))
            def _():
                along(kind, way, hop).wait_recv()
                if hop + 1 < depth - 1:
                    @pl.when(along_valid(way, hop + 1))
                    def _():
                        along(kind, way, hop + 1).start()
                for copy in sideways(kind, 1 + 2 * hop + way, level - sign * (hop + 1)):
                    copy.start()

    def gather_rest(kind):
        for copy in sideways(kind, 0, level):
            copy.wait()
        for hop in range(depth - 1):
            for way in range(2):
                sign = 1 - 2 * way

                @pl.when(along_valid(way, hop))
                def _():
                    along(kind, way, hop).wait_send()

                @pl.when(arrives_valid(way, hop))
                def _():
                    for copy in sideways(kind, 1 + 2 * hop + way, level - sign * (hop + 1)):
                        copy.wait()

    loads[0].wait()
    gather_along(0)
    gather_sideways(0)

    normed = (conv_ref[...].astype(F32) - mean_col) * rstd_col
    pre_act = normed * gain_ref[...] + shift_ref[...]
    act_sigmoid = jax.nn.sigmoid(pre_act)
    gathered[group, proj_rows : proj_rows + tokens, :] = (pre_act * act_sigmoid).astype(BF)
    gather_sideways(1)
    normed_s[...] = normed
    slope_s[...] = act_sigmoid * (1.0 + pre_act * (1.0 - act_sigmoid)) * gain_ref[...]
    back_place = lax.broadcasted_iota(jnp.int32, (tokens, slots), 1).astype(F32)
    back = None
    for choice in range(2):
        same = jnp.where(named_line[0] == named_col[choice], 1.0, 0.0) + jnp.where(
            named_line[1] == named_col[choice], 1.0, 0.0
        )
        rank = jnp.sum(jnp.where(over_iota < down_iota, same, 0.0), axis=1, keepdims=True)
        match = back_place == named_col[choice] * float(cap) + rank
        back = match if back is None else back | match
    chosen_back[...] = jnp.where(back, 1.0, 0.0).astype(BF)

    def of_chunk(part_index):
        return slice(chunks[part_index][0] * cap, chunks[part_index][1] * cap)

    def activate(part_index):
        here = of_chunk(part_index)
        step_rows = 64
        count = here.stop - here.start

        def body(index, carry):
            there = tile(index, step_rows)
            gate_pre, up_pre, hidden_grad = (
                work_a[there, 0:count], work_b[there, 0:count], work_c[there, 0:count]
            )
            gate_sigmoid = jax.nn.sigmoid(gate_pre)
            gate_active = gate_pre * gate_sigmoid
            hid[there, here] = (gate_active * up_pre).astype(BF)
            upg[there, here] = (hidden_grad * gate_active).astype(BF)
            gtg[there, here] = (
                hidden_grad * up_pre * (gate_sigmoid * (1.0 + gate_pre * (1.0 - gate_sigmoid)))
            ).astype(BF)
            return carry

        lax.fori_loop(0, hidden_units // step_rows, body, 0)

    def partial_columns(part_index, lane_index):
        here = of_chunk(part_index)
        there = tile(lane_index, width)
        value = tn(gtg[:, here], gate_w[:, there]) + tn(upg[:, here], up_w[:, there])
        part[here, there] = value.astype(BF)

    swaps, homeward, back_across = ({}, {}, {})

    def swap(part_index, turn):
        away = flipped(lane, 2 * turn + 1)
        here = pl.ds(chunks[part_index][0] * cap, (chunks[part_index][1] - chunks[part_index][0]) * cap)
        swaps[part_index, turn] = go(remote(
            part.at[here, tile(away, width)], half.at[turn, here],
            sw_s.at[part_index, turn], sw_r.at[part_index, turn], partner,
        ))

    def partials(part_index):
        for turn in [*range(1, chips), 0]:
            partial_columns(part_index, flipped(lane, 2 * turn + 1))
            swap(part_index, turn)
            partial_columns(part_index, flipped(lane, 2 * turn))

    def chip_sums(part_index):
        for turn in range(1, chips):
            away = flipped(lane, 2 * turn)
            swaps[part_index, turn].wait_recv()
            for step in range(*chunks[part_index]):
                here = slice(step * cap, (step + 1) * cap)
                summed[turn - 1, here, :] = (
                    part[here, tile(away, width)].astype(F32) + half[turn, here, :].astype(F32)
                ).astype(BF)
                back_across[step, turn] = go(remote(
                    summed.at[turn - 1, pl.ds(step * cap, cap)], arrived.at[turn - 1, pl.ds(step * cap, cap)],
                    cy_s.at[step, turn], cy_r.at[step, turn], (group, away),
                ))

    def send_home(part_index):
        swaps[part_index, 0].wait_recv()
        for step in range(*chunks[part_index]):
            here = slice(step * cap, (step + 1) * cap)
            value = part[here, mine].astype(F32) + half[0, here, :].astype(F32)
            for turn in range(1, chips):
                back_across[step, turn].wait_recv()
                value = value + arrived[turn - 1, here, :].astype(F32)
            if step:
                total[here, :] = value.astype(BF)
                homeward[step] = go(remote(
                    total.at[pl.ds(step * cap, cap)], returned.at[pl.ds(step * cap, cap)],
                    csp_s.at[step], csp_r.at[step], (flipped(group, step), lane),
                ))
            else:
                returned[here, :] = value.astype(BF)

    def first_matmuls(part_index, between):
        here = of_chunk(part_index)
        count = here.stop - here.start
        for work, weight, source in ((work_a, gate_w, 0), (work_b, up_w, 0), (work_c, down_w, 1)):
            work[:, 0:count] = nt(weight[...], rows[source, here, :])
            between.pop(0)()

    def advance(low, high):
        for step in range(low, high):
            dispatched[step].wait_recv()
            forward(step)
            relay(step - 1)

    edge = chunks[0][1]
    advance(1, edge)
    middle = (edge + groups) // 2
    for step in range(edge, middle):
        dispatched[step].wait_recv()
        forward(step)
    relay(edge - 1)
    for step in range(edge):
        for turn in range(chips):
            shared[step, turn].wait_recv()
    for copy in loads[1:]:
        copy.wait()

    def last_forward():
        for step in range(middle, groups):
            dispatched[step].wait_recv()
            forward(step)

    def nothing():
        return None

    first_matmuls(0, [last_forward, nothing, nothing])
    activate(0)
    for step in range(edge, groups):
        relay(step)
    partials(0)
    gather_hop(0, 0)
    chip_sums(0)
    for step in range(edge, groups):
        for turn in range(chips):
            shared[step, turn].wait_recv()
    first_matmuls(1, [nothing, lambda: send_home(0), nothing])
    activate(1)
    partials(1)
    gather_hop(0, 1)
    chip_sums(1)
    for hop in range(2, depth - 1):
        gather_hop(0, hop)
    send_home(1)
    gather_along(1)

    span = min(channels, 512)

    def down_tile(index, carry):
        there = tile(index, span)
        gdown_ref[0, :, there] = nn(hid[...], rows[1, :, there]).astype(BF)
        return carry

    def up_tile(index, carry):
        there = tile(index, span)
        gup_ref[0, :, there] = nn(upg[...], rows[0, :, there]).astype(BF)
        return carry

    lax.fori_loop(0, channels // span, down_tile, 0)
    lax.fori_loop(0, channels // span, up_tile, 0)

    for step in range(1, groups):
        homeward[step].wait_recv()
    picked = nn(chosen_back[...], returned[...])
    own_stream = (cot_ref[...].astype(F32) + picked).astype(BF)
    gstream_ref[...] = own_stream
    mix[:, mine] = own_stream
    tp_across = {}
    for turn in range(1, chips):
        tp_across[turn] = go(remote(
            mix.at[:, mine], mix.at[:, mine], ty_s.at[turn], ty_r.at[turn], (group, flipped(lane, 2 * turn))
        ))
    tp_shared = {0: go(remote(mix.at[:, mine], mix.at[:, mine], tc_s.at[0], tc_r.at[0], partner))}
    for turn in range(1, chips):
        tp_across[turn].wait_recv()
        theirs = tile(flipped(lane, 2 * turn), width)
        tp_shared[turn] = go(remote(
            mix.at[:, theirs], mix.at[:, theirs], tc_s.at[turn], tc_r.at[turn], partner
        ))
    for turn in range(chips):
        tp_shared[turn].wait_recv()

    share = channels // groups
    piece_width = pieces.shape[3]
    quarter = tokens // 4
    place_of_four = lax.rem(lane, 4)

    def piece_of(owner):
        if share == piece_width:
            return tile(owner, share)
        return tile(lax.div(owner * share, piece_width), piece_width)

    travelling, piece_across, piece_shared = ({}, {}, {})
    for step in range(1, groups):
        owner = flipped(group, step)
        travelling[step] = go(remote(
            mix.at[tile(place_of_four, quarter), piece_of(owner)], pieces.at[step, place_of_four],
            p_s.at[step], p_r.at[step], (owner, lane),
        ))

    def piece_forward(step):
        travelling[step].wait_recv()
        here = pieces.at[step, place_of_four]
        piece_across[step] = go(remote(
            here, here, py_s.at[step], py_r.at[step], (group, flipped(lane, 2))
        ))
        piece_shared[step, 0] = go(remote(here, here, pc_s.at[step, 0], pc_r.at[step, 0], partner))

    def piece_relay(step):
        piece_across[step].wait_recv()
        here = pieces.at[step, flipped(place_of_four, 2)]
        piece_shared[step, 1] = go(remote(here, here, pc_s.at[step, 1], pc_r.at[step, 1], partner))

    gather_rest(0)
    whole_proj = gathered[:, 0:proj_rows, :].reshape(groups * proj_rows, width)
    normed_grad = nn(mix[...], whole_proj) * slope_s[...]
    weighted = normed_grad * normed_s[...]
    ones = jnp.ones((16, width), BF)

    def line_sum(value):
        high = value.astype(BF)
        low = (value - high.astype(F32)).astype(BF)
        return nt(ones, high) + nt(ones, low)

    line = lax.broadcasted_iota(jnp.int32, (16, tokens), 0)
    own_stat = jnp.where(line == 0, line_sum(normed_grad), line_sum(weighted))
    stat_out[...] = own_stat
    stats = []
    for step in range(1, lanes):
        stats.append(go(remote(
            stat_out, stat_in.at[step], st_s.at[step], st_r.at[step], (group, flipped(lane, step))
        )))
    for step in range(1, groups // 2):
        piece_forward(step)
    gather_hop(1, 0)
    all_stat = own_stat
    for step in range(1, lanes):
        stats[step - 1].wait_recv()
        all_stat = all_stat + stat_in[step]
    all_stat = all_stat * (1.0 / channels)
    high = all_stat.astype(BF)
    middle = (all_stat - high.astype(F32)).astype(BF)
    low = (all_stat - high.astype(F32) - middle.astype(F32)).astype(BF)
    pick = lax.broadcasted_iota(jnp.int32, (16, width), 0)

    def spread_line(number):
        chooser = jnp.where(pick == number, 1.0, 0.0).astype(BF)
        return tn(high, chooser) + tn(middle, chooser) + tn(low, chooser)

    first_line, second_line = (spread_line(0), spread_line(1))
    rim = ext.shape[0] - tokens

    def halo():
        return remote(
            ext.at[pl.ds(0, rim)], ext.at[pl.ds(tokens, rim)], halo_s, halo_r, (group - 1, lane)
        )

    def conv_gradient(here):
        ext[here, :] = rstd_col[here] * (
            normed_grad[here] - first_line[here] - normed_s[here, :] * second_line[here]
        )

    conv_gradient(slice(0, rim))

    @pl.when(group > 0)
    def _():
        halo().start()

    conv_gradient(slice(rim, tokens))
    for step in range(groups // 2, groups):
        piece_forward(step)
    for hop in range(1, depth - 1):
        gather_hop(1, hop)
    for step in range(1, groups):
        piece_relay(step)

    @pl.when(group < groups - 1)
    def _():
        halo().wait_recv()

    @pl.when(group == groups - 1)
    def _():
        ext[tokens : tokens + rim, :] = jnp.zeros((rim, width), F32)

    def conv_tile(index, carry):
        there = tile(index, 128)
        chunk = 64
        for start in range(0, tokens, chunk):
            value = jnp.zeros((chunk, 128), F32)
            for lag in range(lag_count):
                value = value + taps_ref[lag : lag + 1, there] * ext[start + lag : start + lag + chunk, there]
            gconv_ref[start : start + chunk, there] = value.astype(BF)
        return carry

    lax.fori_loop(0, width // 128, conv_tile, 0)

    def piece_value(value):
        if share == piece_width:
            return value
        per = piece_width // share
        which = lax.rem(group, per)
        result = value[:, 0:share]
        for index in range(1, per):
            result = jnp.where(which == index, value[:, index * share : (index + 1) * share], result)
        return result

    gather_rest(1)
    gproj = tn(piece_value(mix[:, piece_of(group)]), gathered[group, proj_rows : proj_rows + tokens, :])
    for step in range(1, groups):
        for turn in range(2):
            piece_shared[step, turn].wait_recv()
        owner = flipped(group, step)
        gproj = gproj + tn(piece_value(pieces[step].reshape(tokens, piece_width)), gathered[owner, proj_rows : proj_rows + tokens, :])
    gproj_ref[...] = gproj

    @pl.when(group > 0)
    def _():
        halo().wait_send()

    for copy in outgoing:
        copy.wait_send()


def on_device(
    moe_in, cotangent, routes, route_weight, w_gate, w_up, w_down,
    conv_pre, norm_mean, norm_rstd, ln_gain, ln_shift, taps, w_proj,
):
    groups, lanes = (lax.axis_size("sp"), lax.axis_size("tp"))
    chips = lanes // 2
    across = 1 << (groups.bit_length() // 2 - 1)
    depth = groups // across
    tokens, width = moe_in.shape
    channels = width * lanes
    hidden_units = w_gate.shape[1]
    cap = (5 * tokens // (2 * groups) + 15) // 16 * 16
    slots = groups * cap
    chunk_rows = 3 * groups // 4 * cap
    proj_rows = w_proj.shape[0]
    share = channels // groups
    piece_width = max(share, 128)
    rim = (taps.shape[0] - 1 + 7) // 8 * 8
    vmem_limit = 48 * 1024 * 1024
    dma = pltpu.SemaphoreType.DMA
    vmem = pltpu.VMEM
    others = max(1, chips - 1)
    inside = pl.BlockSpec(memory_space=pltpu.VMEM)
    outside = pl.BlockSpec(memory_space=pl.ANY)
    return pl.pallas_call(
        functools.partial(layer_kernel, groups, lanes, across),
        out_shape=(
            vmem(w_up.shape, BF),
            vmem(w_down.shape, BF),
            vmem((tokens, width), BF),
            vmem((proj_rows, width), F32),
            vmem((tokens, width), BF),
        ),
        in_specs=[inside] * 10 + [outside] * 4,
        out_specs=(inside,) * 5,
        scratch_shapes=[
            vmem((hidden_units, channels), BF), vmem((hidden_units, channels), BF), vmem((hidden_units, channels), BF),
            vmem((2, slots, width), BF), vmem((2, slots, channels), BF),
            vmem((hidden_units, chunk_rows), F32), vmem((hidden_units, chunk_rows), F32), vmem((hidden_units, chunk_rows), F32),
            vmem((hidden_units, slots), BF), vmem((hidden_units, slots), BF), vmem((hidden_units, slots), BF),
            vmem((slots, channels), BF), vmem((chips, slots, width), BF),
            vmem((others, slots, width), BF), vmem((others, slots, width), BF),
            vmem((slots, width), BF), vmem((slots, width), BF), vmem((tokens, slots), BF),
            vmem((groups, proj_rows + tokens, width), BF), vmem((tokens, channels), BF),
            vmem((groups, 4, tokens // 4, piece_width), BF),
            vmem((128, (tokens + 127) // 128 * 128), F32), vmem((tokens, width), F32), vmem((tokens, width), F32),
            vmem((16, tokens), F32), vmem((lanes, 16, tokens), F32), vmem((tokens + rim, width), F32),
            dma((4,)), dma((groups,)), dma((groups,)),
            dma((groups, chips)), dma((groups, chips)), dma((groups, chips)), dma((groups, chips)),
            dma((2, chips)), dma((2, chips)), dma((groups, chips)), dma((groups, chips)),
            dma((groups,)), dma((groups,)),
            dma((2, 2, depth)), dma((2, 2, depth)), dma((2, 2 * depth, across)), dma((2, 2 * depth, across)),
            dma((chips,)), dma((chips,)), dma((chips,)), dma((chips,)),
            dma((groups,)), dma((groups,)), dma((groups,)), dma((groups,)), dma((groups, 2)), dma((groups, 2)),
            dma((lanes,)), dma((lanes,)), dma, dma,
        ],
        compiler_params=pltpu.CompilerParams(
            collective_id=1, has_side_effects=True, vmem_limit_bytes=vmem_limit
        ),
    )(
        moe_in, cotangent, routes.T, route_weight.T, norm_mean[None, :], norm_rstd[None, :], conv_pre, ln_gain[None, :], ln_shift[None, :], taps,
        w_gate, w_up, w_down, w_proj,
    )


def solution(mesh):
    placed = (
        P("sp", "tp"), P("sp", "tp"), P("sp", None), P("sp", None),
        P("sp", "tp", None), P("sp", "tp", None), P("sp", "tp", None),
        P("sp", "tp"), P("sp"), P("sp"), P("tp"), P("tp"), P(None, "tp"), P("sp", "tp"),
    )
    return jax.shard_map(
        on_device,
        mesh=mesh,
        in_specs=placed,
        out_specs=(
            P("sp", "tp", None), P("sp", "tp", None), P("sp", "tp"), P("sp", "tp"), P("sp", "tp"),
        ),
        check_vma=False,
    )
```

```python
import functools

import jax
import jax.numpy as jnp
from jax import lax
from jax.experimental import pallas as pl
from jax.experimental.pallas import tpu as pltpu
from jax.sharding import PartitionSpec as P

MESH = pl.DeviceIdType.MESH
BF = jnp.bfloat16
F32 = jnp.float32


def flipped(index, step):
    value, bit = index, 1
    while bit <= step:
        if step & bit:
            value = value + bit * (1 - 2 * lax.rem(lax.div(index, bit), 2))
        bit *= 2
    return value


def tile(index, size):
    return pl.ds(pl.multiple_of(index * size, size), size)


def nn(left, right):
    return lax.dot_general(left, right, (((1,), (0,)), ((), ())), preferred_element_type=F32)


def nt(left, right):
    return lax.dot_general(left, right, (((1,), (1,)), ((), ())), preferred_element_type=F32)


def tn(left, right):
    return lax.dot_general(left, right, (((0,), (0,)), ((), ())), preferred_element_type=F32)


def layer_kernel(
    groups, lanes, across,
    moe_ref, cot_ref, route_ref, weight_ref, mean_ref, rstd_ref, conv_ref, gain_ref, shift_ref, taps_ref,
    gate_hbm, up_hbm, down_hbm, proj_hbm,
    gup_ref, gdown_ref, gstream_ref, gproj_ref, gconv_ref,
    gate_w, up_w, down_w, send, rows, work_a, work_b, work_c, hid, upg, gtg,
    part, half, summed, arrived, total, returned, chosen_back, gathered, mix, pieces,
    lines_s, normed_s, slope_s, stat_out, stat_in, ext,
    load_sem, dsp_s, dsp_r, dy_s, dy_r, dc_s, dc_r, sw_s, sw_r, cy_s, cy_r, csp_s, csp_r,
    az_s, az_r, ax_s, ax_r, ty_s, ty_r, tc_s, tc_r, p_s, p_r, py_s, py_r, pc_s, pc_r, st_s, st_r, halo_s, halo_r,
):
    group, lane = (lax.axis_index("sp"), lax.axis_index("tp"))
    chips = lanes // 2
    depth = groups // across
    chip, core = (lax.div(lane, 2), lax.rem(lane, 2))
    level, column = (lax.div(group, across), lax.rem(group, across))
    tokens, width = moe_ref.shape
    channels = width * lanes
    hidden_units = gate_w.shape[0]
    slots = groups * (rows.shape[1] // groups)
    cap = slots // groups
    chunks = ((0, groups // 2), (groups // 2, 3 * groups // 4), (3 * groups // 4, groups))
    proj_rows = proj_hbm.shape[0]
    lag_count = taps_ref.shape[0]
    partner = (group, flipped(lane, 1))
    mine = tile(lane, width)

    barrier = pltpu.get_barrier_semaphore()
    for step in range(1, groups):
        pl.semaphore_signal(barrier, inc=1, device_id=(flipped(group, step), lane), device_id_type=MESH)
    for step in range(1, lanes):
        pl.semaphore_signal(barrier, inc=1, device_id=(group, flipped(lane, step)), device_id_type=MESH)

    def remote(source, target, sends, recvs, device):
        return pltpu.make_async_remote_copy(
            src_ref=source, dst_ref=target, send_sem=sends, recv_sem=recvs,
            device_id=device, device_id_type=MESH,
        )

    loads = [
        pltpu.make_async_copy(proj_hbm, gathered.at[group, pl.ds(0, proj_rows)], load_sem.at[0]),
        pltpu.make_async_copy(gate_hbm.at[0], gate_w, load_sem.at[1]),
        pltpu.make_async_copy(up_hbm.at[0], up_w, load_sem.at[2]),
        pltpu.make_async_copy(down_hbm.at[0], down_w, load_sem.at[3]),
    ]
    for copy in loads:
        copy.start()

    lines_s[...] = jnp.zeros(lines_s.shape, F32)
    lines_s[0:2, 0:tokens] = (route_ref[...] ^ group).astype(F32)
    lines_s[2:3, 0:tokens] = mean_ref[...]
    lines_s[3:4, 0:tokens] = rstd_ref[...]
    named_line = (lines_s[0:1, 0:tokens], lines_s[1:2, 0:tokens])
    weight_line = (weight_ref[0:1, :], weight_ref[1:2, :])
    columns = lines_s[...].T
    named_col = (columns[0:tokens, 0:1], columns[0:tokens, 1:2])
    mean_col, rstd_col = (columns[0:tokens, 2:3], columns[0:tokens, 3:4])
    down_iota = lax.broadcasted_iota(jnp.int32, (tokens, tokens), 0)
    over_iota = lax.broadcasted_iota(jnp.int32, (tokens, tokens), 1)
    targets = []
    for choice in range(2):
        same = jnp.where(named_col[0] == named_line[choice], 1.0, 0.0) + jnp.where(
            named_col[1] == named_line[choice], 1.0, 0.0
        )
        rank = jnp.sum(jnp.where(down_iota < over_iota, same, 0.0), axis=0, keepdims=True)
        targets.append(named_line[choice] * float(cap) + rank)

    def fill(low, high):
        here = slice(low * cap, high * cap)
        count = (high - low) * cap
        place = lax.broadcasted_iota(jnp.int32, (count, tokens), 0).astype(F32) + float(low * cap)
        first, second = (place == targets[0], place == targets[1])
        slot_weight = jnp.sum(
            jnp.where(first, weight_line[0], 0.0) + jnp.where(second, weight_line[1], 0.0),
            axis=1, keepdims=True,
        )
        chosen = jnp.where(first | second, 1.0, 0.0).astype(BF)
        send[0, here, :] = nn(chosen, moe_ref[...]).astype(BF)
        send[1, here, :] = (slot_weight * nn(chosen, cot_ref[...])).astype(BF)

    fill(0, groups // 2)
    rows[0, 0:cap, mine] = send[0, 0:cap, :]
    rows[1, 0:cap, mine] = send[1, 0:cap, :]

    pl.semaphore_wait(barrier, groups + lanes - 2)

    def at_slot(step, lane_index):
        return rows.at[:, pl.ds(step * cap, cap), tile(lane_index, width)]

    outgoing = []

    def go(copy):
        copy.start()
        outgoing.append(copy)
        return copy

    dispatched, crossed, shared = ({}, {}, {})

    def forward(step):
        for turn in range(1, chips):
            crossed[step, turn] = go(remote(
                at_slot(step, lane), at_slot(step, lane), dy_s.at[step, turn - 1], dy_r.at[step, turn - 1],
                (group, flipped(lane, 2 * turn)),
            ))
        shared[step, 0] = go(remote(
            at_slot(step, lane), at_slot(step, lane), dc_s.at[step, 0], dc_r.at[step, 0], partner
        ))

    def relay(step):
        for turn in range(1, chips):
            crossed[step, turn].wait_recv()
            peer = flipped(lane, 2 * turn)
            shared[step, turn] = go(remote(
                at_slot(step, peer), at_slot(step, peer), dc_s.at[step, turn], dc_r.at[step, turn], partner
            ))

    def dispatch(step):
        dispatched[step] = go(remote(
            send.at[:, pl.ds(step * cap, cap)], at_slot(step, lane),
            dsp_s.at[step], dsp_r.at[step], (flipped(group, step), lane),
        ))

    forward(0)
    for step in range(1, groups // 2):
        dispatch(step)
    fill(groups // 2, groups)
    for step in range(groups // 2, 3 * groups // 4):
        dispatch(step)

    bounds = ((0, proj_rows), (proj_rows, tokens))

    def block(owner_level, owner_column, kind):
        return gathered.at[owner_level * across + owner_column, pl.ds(bounds[kind][0], bounds[kind][1])]

    def along(kind, way, hop):
        sign = 1 - 2 * way
        source_level = level - sign * hop
        here = block(source_level, column, kind)
        return remote(
            here, here, az_s.at[kind, way, hop], az_r.at[kind, way, hop],
            ((level + sign) * across + column, lane),
        )

    def along_valid(way, hop):
        if way == 0:
            return (level - hop >= 0) & (level + 1 < depth)
        return (level + hop < depth) & (level - 1 >= 0)

    def arrives_valid(way, hop):
        if way == 0:
            return level - 1 - hop >= 0
        return level + 1 + hop < depth

    def sideways(kind, event, owner_level):
        copies = []
        for turn in range(1, across):
            here = block(owner_level, column, kind)
            copies.append(remote(
                here, here, ax_s.at[kind, event, turn - 1], ax_r.at[kind, event, turn - 1],
                (level * across + flipped(column, turn), lane),
            ))
        return copies

    def over_middle(way, source_level, wanted):
        edge_level = depth // 2 - 1 + way
        return (source_level == edge_level) if wanted else (source_level != edge_level)

    def gather_along(kind, middle):
        for way in range(2):
            @pl.when(along_valid(way, 0) & over_middle(way, level, middle))
            def _():
                along(kind, way, 0).start()

    def gather_sideways(kind):
        for copy in sideways(kind, 0, level):
            copy.start()

    def gather_hop(kind, hop, middle=None):
        for way in range(2):
            sign = 1 - 2 * way
            due = arrives_valid(way, hop)
            if middle is not None:
                due = due & over_middle(way, level - sign, middle)

            @pl.when(due)
            def _():
                along(kind, way, hop).wait_recv()
                if hop + 1 < depth - 1:
                    @pl.when(along_valid(way, hop + 1))
                    def _():
                        along(kind, way, hop + 1).start()
                for copy in sideways(kind, 1 + 2 * hop + way, level - sign * (hop + 1)):
                    copy.start()

    def gather_rest(kind):
        for copy in sideways(kind, 0, level):
            copy.wait()
        for hop in range(depth - 1):
            for way in range(2):
                sign = 1 - 2 * way

                @pl.when(along_valid(way, hop))
                def _():
                    along(kind, way, hop).wait_send()

                @pl.when(arrives_valid(way, hop))
                def _():
                    for copy in sideways(kind, 1 + 2 * hop + way, level - sign * (hop + 1)):
                        copy.wait()


    normed = (conv_ref[...].astype(F32) - mean_col) * rstd_col
    pre_act = normed * gain_ref[...] + shift_ref[...]
    act_sigmoid = jax.nn.sigmoid(pre_act)
    gathered[group, proj_rows : proj_rows + tokens, :] = (pre_act * act_sigmoid).astype(BF)
    normed_s[...] = normed
    slope_s[...] = act_sigmoid * (1.0 + pre_act * (1.0 - act_sigmoid)) * gain_ref[...]
    back_place = lax.broadcasted_iota(jnp.int32, (tokens, slots), 1).astype(F32)
    back = None
    for choice in range(2):
        same = jnp.where(named_line[0] == named_col[choice], 1.0, 0.0) + jnp.where(
            named_line[1] == named_col[choice], 1.0, 0.0
        )
        rank = jnp.sum(jnp.where(over_iota < down_iota, same, 0.0), axis=1, keepdims=True)
        match = back_place == named_col[choice] * float(cap) + rank
        back = match if back is None else back | match
    chosen_back[...] = jnp.where(back, 1.0, 0.0).astype(BF)

    def of_chunk(part_index):
        return slice(chunks[part_index][0] * cap, chunks[part_index][1] * cap)

    def activate(part_index):
        here = of_chunk(part_index)
        step_rows = 64
        count = here.stop - here.start

        def body(index, carry):
            there = tile(index, step_rows)
            gate_pre, up_pre, hidden_grad = (
                work_a[there, 0:count], work_b[there, 0:count], work_c[there, 0:count]
            )
            gate_sigmoid = jax.nn.sigmoid(gate_pre)
            gate_active = gate_pre * gate_sigmoid
            hid[there, here] = (gate_active * up_pre).astype(BF)
            upg[there, here] = (hidden_grad * gate_active).astype(BF)
            gtg[there, here] = (
                hidden_grad * up_pre * (gate_sigmoid * (1.0 + gate_pre * (1.0 - gate_sigmoid)))
            ).astype(BF)
            return carry

        lax.fori_loop(0, hidden_units // step_rows, body, 0)

    def partial_columns(part_index, lane_index):
        here = of_chunk(part_index)
        there = tile(lane_index, width)
        value = tn(gtg[:, here], gate_w[:, there]) + tn(upg[:, here], up_w[:, there])
        part[here, there] = value.astype(BF)

    swaps, homeward, back_across = ({}, {}, {})

    def swap(part_index, turn):
        away = flipped(lane, 2 * turn + 1)
        here = pl.ds(chunks[part_index][0] * cap, (chunks[part_index][1] - chunks[part_index][0]) * cap)
        swaps[part_index, turn] = go(remote(
            part.at[here, tile(away, width)], half.at[turn, here],
            sw_s.at[part_index, turn], sw_r.at[part_index, turn], partner,
        ))

    def partials(part_index, between):
        for turn in [*range(1, chips), 0]:
            partial_columns(part_index, flipped(lane, 2 * turn + 1))
            swap(part_index, turn)
            partial_columns(part_index, flipped(lane, 2 * turn))
            if turn == 1:
                between()

    def chip_sums(part_index):
        for turn in range(1, chips):
            away = flipped(lane, 2 * turn)
            swaps[part_index, turn].wait_recv()
            for step in range(*chunks[part_index]):
                here = slice(step * cap, (step + 1) * cap)
                summed[turn - 1, here, :] = (
                    part[here, tile(away, width)].astype(F32) + half[turn, here, :].astype(F32)
                ).astype(BF)
                back_across[step, turn] = go(remote(
                    summed.at[turn - 1, pl.ds(step * cap, cap)], arrived.at[turn - 1, pl.ds(step * cap, cap)],
                    cy_s.at[step, turn - 1], cy_r.at[step, turn - 1], (group, away),
                ))

    def send_home(part_index):
        swaps[part_index, 0].wait_recv()
        for step in range(*chunks[part_index]):
            here = slice(step * cap, (step + 1) * cap)
            value = part[here, mine].astype(F32) + half[0, here, :].astype(F32)
            for turn in range(1, chips):
                back_across[step, turn].wait_recv()
                value = value + arrived[turn - 1, here, :].astype(F32)
            if step:
                total[here, :] = value.astype(BF)
                homeward[step] = go(remote(
                    total.at[pl.ds(step * cap, cap)], returned.at[pl.ds(step * cap, cap)],
                    csp_s.at[step], csp_r.at[step], (flipped(group, step), lane),
                ))
            else:
                returned[here, :] = value.astype(BF)

    def first_matmuls(part_index, between):
        here = of_chunk(part_index)
        count = here.stop - here.start
        for work, weight, source in ((work_a, gate_w, 0), (work_b, up_w, 0), (work_c, down_w, 1)):
            work[:, 0:count] = nt(weight[...], rows[source, here, :])
            between.pop(0)()

    def advance(low, high):
        for step in range(low, high):
            dispatched[step].wait_recv()
            forward(step)
            if step % 2:
                dispatch(3 * groups // 4 + step // 2)
            relay(step - 1)

    def pass_on(low, high):
        for step in range(low, high):
            dispatched[step].wait_recv()
            forward(step)

    def relays(low, high):
        for step in range(low, high):
            relay(step)

    def complete(part_index):
        for step in range(*chunks[part_index]):
            for turn in range(chips):
                shared[step, turn].wait_recv()

    def nothing():
        return None

    first_edge, second_edge = (chunks[0][1], chunks[1][1])
    first_half, second_half = ((first_edge + second_edge) // 2, (second_edge + groups) // 2)
    advance(1, first_edge)
    loads[0].wait()
    for kind in range(2):
        gather_along(kind, False)
        gather_sideways(kind)
    relays(first_edge - 1, first_edge)
    complete(0)
    pass_on(first_edge, first_half)
    for copy in loads[1:]:
        copy.wait()
    gather_along(0, True)
    first_matmuls(0, [lambda: pass_on(first_half, second_edge), nothing, lambda: pass_on(second_edge, second_half)])
    activate(0)
    relays(first_edge, first_half)

    def rest_of_dispatch():
        pass_on(second_half, groups)
        relays(first_half, second_edge)

    partials(0, rest_of_dispatch)
    relays(second_edge, second_half)
    chip_sums(0)
    gather_hop(0, 0, False)
    gather_along(1, True)
    gather_hop(1, 0, False)
    complete(1)
    first_matmuls(1, [nothing, nothing, nothing])
    relays(second_half, groups)
    gather_hop(0, 0, True)
    activate(1)
    partials(1, nothing)
    chip_sums(1)
    complete(2)
    first_matmuls(2, [nothing, nothing, nothing])
    gather_hop(0, 1)
    send_home(0)
    activate(2)
    send_home(1)
    gather_hop(1, 0, True)
    partials(2, nothing)
    chip_sums(2)
    send_home(2)

    span = min(channels, 512)

    def down_tile(index, carry):
        there = tile(index, span)
        gdown_ref[0, :, there] = nn(hid[...], rows[1, :, there]).astype(BF)
        return carry

    def up_tile(index, carry):
        there = tile(index, span)
        gup_ref[0, :, there] = nn(upg[...], rows[0, :, there]).astype(BF)
        return carry

    lax.fori_loop(0, channels // span, down_tile, 0)
    lax.fori_loop(0, channels // span, up_tile, 0)
    for hop in range(2, depth - 1):
        gather_hop(0, hop)
    gather_hop(1, 1, True)

    for step in range(1, groups):
        homeward[step].wait_recv()
    picked = nn(chosen_back[...], returned[...])
    own_stream = (cot_ref[...].astype(F32) + picked).astype(BF)
    gstream_ref[...] = own_stream
    mix[:, mine] = own_stream
    tp_across = {}
    for turn in range(1, chips):
        tp_across[turn] = go(remote(
            mix.at[:, mine], mix.at[:, mine], ty_s.at[turn], ty_r.at[turn], (group, flipped(lane, 2 * turn))
        ))
    tp_shared = {0: go(remote(mix.at[:, mine], mix.at[:, mine], tc_s.at[0], tc_r.at[0], partner))}
    for turn in range(1, chips):
        tp_across[turn].wait_recv()
        theirs = tile(flipped(lane, 2 * turn), width)
        tp_shared[turn] = go(remote(
            mix.at[:, theirs], mix.at[:, theirs], tc_s.at[turn], tc_r.at[turn], partner
        ))
    gather_hop(1, 1, False)
    for turn in range(chips):
        tp_shared[turn].wait_recv()

    share = channels // groups
    piece_width = pieces.shape[3]
    quarter = tokens // 4
    place_of_four = lax.rem(lane, 4)

    def piece_of(owner):
        if share == piece_width:
            return tile(owner, share)
        return tile(lax.div(owner * share, piece_width), piece_width)

    travelling, piece_across, piece_shared = ({}, {}, {})
    for step in range(1, groups):
        owner = flipped(group, step)
        travelling[step] = go(remote(
            mix.at[tile(place_of_four, quarter), piece_of(owner)], pieces.at[step, place_of_four],
            p_s.at[step], p_r.at[step], (owner, lane),
        ))

    def piece_forward(step):
        travelling[step].wait_recv()
        here = pieces.at[step, place_of_four]
        piece_across[step] = go(remote(
            here, here, py_s.at[step], py_r.at[step], (group, flipped(lane, 2))
        ))
        piece_shared[step, 0] = go(remote(here, here, pc_s.at[step, 0], pc_r.at[step, 0], partner))

    def piece_relay(step):
        piece_across[step].wait_recv()
        here = pieces.at[step, flipped(place_of_four, 2)]
        piece_shared[step, 1] = go(remote(here, here, pc_s.at[step, 1], pc_r.at[step, 1], partner))

    gather_rest(0)
    whole_proj = gathered[:, 0:proj_rows, :].reshape(groups * proj_rows, width)
    normed_grad = nn(mix[...], whole_proj) * slope_s[...]
    weighted = normed_grad * normed_s[...]
    ones = jnp.ones((16, width), BF)

    def line_sum(value):
        high = value.astype(BF)
        low = (value - high.astype(F32)).astype(BF)
        return nt(ones, high) + nt(ones, low)

    line = lax.broadcasted_iota(jnp.int32, (16, tokens), 0)
    own_stat = jnp.where(line == 0, line_sum(normed_grad), line_sum(weighted))
    stat_out[...] = own_stat
    stats = []
    for step in range(1, lanes):
        stats.append(go(remote(
            stat_out, stat_in.at[step], st_s.at[step], st_r.at[step], (group, flipped(lane, step))
        )))
    all_stat = own_stat
    for step in range(1, lanes):
        stats[step - 1].wait_recv()
        all_stat = all_stat + stat_in[step]
    all_stat = all_stat * (1.0 / channels)
    high = all_stat.astype(BF)
    middle = (all_stat - high.astype(F32)).astype(BF)
    low = (all_stat - high.astype(F32) - middle.astype(F32)).astype(BF)
    pick = lax.broadcasted_iota(jnp.int32, (16, width), 0)

    def spread_line(number):
        chooser = jnp.where(pick == number, 1.0, 0.0).astype(BF)
        return tn(high, chooser) + tn(middle, chooser) + tn(low, chooser)

    first_line, second_line = (spread_line(0), spread_line(1))
    rim = ext.shape[0] - tokens

    def halo():
        return remote(
            ext.at[pl.ds(0, rim)], ext.at[pl.ds(tokens, rim)], halo_s, halo_r, (group - 1, lane)
        )

    def conv_gradient(here):
        ext[here, :] = rstd_col[here] * (
            normed_grad[here] - first_line[here] - normed_s[here, :] * second_line[here]
        )

    conv_gradient(slice(0, rim))

    @pl.when(group > 0)
    def _():
        halo().start()

    conv_gradient(slice(rim, tokens))
    for hop in range(2, depth - 1):
        gather_hop(1, hop)
    for step in range(1, groups):
        piece_forward(step)

    @pl.when(group < groups - 1)
    def _():
        halo().wait_recv()

    @pl.when(group == groups - 1)
    def _():
        ext[tokens : tokens + rim, :] = jnp.zeros((rim, width), F32)

    def conv_tile(index, carry):
        there = tile(index, 128)
        chunk = 64
        for start in range(0, tokens, chunk):
            value = jnp.zeros((chunk, 128), F32)
            for lag in range(lag_count):
                value = value + taps_ref[lag : lag + 1, there] * ext[start + lag : start + lag + chunk, there]
            gconv_ref[start : start + chunk, there] = value.astype(BF)
        return carry

    lax.fori_loop(0, width // 128, conv_tile, 0)

    def piece_value(value):
        if share == piece_width:
            return value
        per = piece_width // share
        which = lax.rem(group, per)
        result = value[:, 0:share]
        for index in range(1, per):
            result = jnp.where(which == index, value[:, index * share : (index + 1) * share], result)
        return result

    for step in range(1, groups):
        piece_relay(step)
    gather_rest(1)
    gproj = tn(piece_value(mix[:, piece_of(group)]), gathered[group, proj_rows : proj_rows + tokens, :])
    for step in range(1, groups):
        for turn in range(2):
            piece_shared[step, turn].wait_recv()
        owner = flipped(group, step)
        gproj = gproj + tn(piece_value(pieces[step].reshape(tokens, piece_width)), gathered[owner, proj_rows : proj_rows + tokens, :])
    gproj_ref[...] = gproj

    @pl.when(group > 0)
    def _():
        halo().wait_send()

    for copy in outgoing:
        copy.wait_send()


def on_device(
    moe_in, cotangent, routes, route_weight, w_gate, w_up, w_down,
    conv_pre, norm_mean, norm_rstd, ln_gain, ln_shift, taps, w_proj,
):
    groups, lanes = (lax.axis_size("sp"), lax.axis_size("tp"))
    chips = lanes // 2
    across = 1 << (groups.bit_length() // 2 - 1)
    depth = groups // across
    tokens, width = moe_in.shape
    channels = width * lanes
    hidden_units = w_gate.shape[1]
    cap = (5 * tokens // (2 * groups) + 15) // 16 * 16
    slots = groups * cap
    proj_rows = w_proj.shape[0]
    share = channels // groups
    piece_width = max(share, 128)
    rim = (taps.shape[0] - 1 + 7) // 8 * 8
    vmem_limit = 48 * 1024 * 1024
    dma = pltpu.SemaphoreType.DMA
    vmem = pltpu.VMEM
    others = max(1, chips - 1)
    inside = pl.BlockSpec(memory_space=pltpu.VMEM)
    outside = pl.BlockSpec(memory_space=pl.ANY)
    results = pl.pallas_call(
        functools.partial(layer_kernel, groups, lanes, across),
        out_shape=(
            vmem(w_up.shape, BF),
            vmem(w_down.shape, BF),
            vmem((tokens, width), BF),
            vmem((proj_rows, width), F32),
            vmem((tokens, width), BF),
        ),
        in_specs=[inside] * 10 + [outside] * 4,
        out_specs=(inside,) * 5,
        scratch_shapes=[
            vmem((hidden_units, channels), BF), vmem((hidden_units, channels), BF), vmem((hidden_units, channels), BF),
            vmem((2, slots, width), BF), vmem((2, slots, channels), BF),
            vmem((hidden_units, slots // 2), F32), vmem((hidden_units, slots // 2), F32), vmem((hidden_units, slots // 2), F32),
            vmem((hidden_units, slots), BF), vmem((hidden_units, slots), BF), vmem((hidden_units, slots), BF),
            vmem((slots, channels), BF), vmem((chips, slots, width), BF),
            vmem((others, slots, width), BF), vmem((others, slots, width), BF),
            vmem((slots, width), BF), vmem((slots, width), BF), vmem((tokens, slots), BF),
            vmem((groups, proj_rows + tokens, width), BF), vmem((tokens, channels), BF),
            vmem((groups, 4, tokens // 4, piece_width), BF),
            vmem((128, (tokens + 127) // 128 * 128), F32), vmem((tokens, width), F32), vmem((tokens, width), F32),
            vmem((16, tokens), F32), vmem((lanes, 16, tokens), F32), vmem((tokens + rim, width), F32),
            dma((4,)), dma((groups,)), dma((groups,)),
            dma((groups, others)), dma((groups, others)), dma((groups, chips)), dma((groups, chips)),
            dma((3, chips)), dma((3, chips)), dma((groups, others)), dma((groups, others)),
            dma((groups,)), dma((groups,)),
            dma((2, 2, depth - 1)), dma((2, 2, depth - 1)),
            dma((2, 2 * depth - 1, across - 1)), dma((2, 2 * depth - 1, across - 1)),
            dma((chips,)), dma((chips,)), dma((chips,)), dma((chips,)),
            dma((groups,)), dma((groups,)), dma((groups,)), dma((groups,)), dma((groups, 2)), dma((groups, 2)),
            dma((lanes,)), dma((lanes,)), dma, dma,
        ],
        compiler_params=pltpu.CompilerParams(
            collective_id=1, has_side_effects=True, vmem_limit_bytes=vmem_limit
        ),
    )(
        moe_in, cotangent, routes.T, route_weight.T, norm_mean[None, :], norm_rstd[None, :], conv_pre, ln_gain[None, :], ln_shift[None, :], taps,
        w_gate, w_up, w_down, w_proj,
    )
    return pl.pallas_call(
        write_kernel,
        out_shape=tuple(jax.ShapeDtypeStruct(result.shape, result.dtype) for result in results),
        in_specs=[inside] * 5,
        out_specs=(outside,) * 5,
        scratch_shapes=[dma((5,))],
        compiler_params=pltpu.CompilerParams(vmem_limit_bytes=16 * 1024 * 1024),
    )(*results)


def write_kernel(*refs):
    copies = [pltpu.make_async_copy(refs[index], refs[5 + index], refs[10].at[index]) for index in range(5)]
    for copy in copies:
        copy.start()
    for copy in copies:
        copy.wait()


def solution(mesh):
    placed = (
        P("sp", "tp"), P("sp", "tp"), P("sp", None), P("sp", None),
        P("sp", "tp", None), P("sp", "tp", None), P("sp", "tp", None),
        P("sp", "tp"), P("sp"), P("sp"), P("tp"), P("tp"), P(None, "tp"), P("sp", "tp"),
    )
    return jax.shard_map(
        on_device,
        mesh=mesh,
        in_specs=placed,
        out_specs=(
            P("sp", "tp", None), P("sp", "tp", None), P("sp", "tp"), P("sp", "tp"), P("sp", "tp"),
        ),
        check_vma=False,
    )
```

```python
import functools

import jax
import jax.numpy as jnp
from jax import lax
from jax.experimental import pallas as pl
from jax.experimental.pallas import tpu as pltpu
from jax.sharding import PartitionSpec as P

MESH = pl.DeviceIdType.MESH
BF = jnp.bfloat16
F32 = jnp.float32


def flipped(index, step):
    value, bit = index, 1
    while bit <= step:
        if step & bit:
            value = value + bit * (1 - 2 * lax.rem(lax.div(index, bit), 2))
        bit *= 2
    return value


def tile(index, size):
    return pl.ds(pl.multiple_of(index * size, size), size)


def nn(left, right):
    return lax.dot_general(left, right, (((1,), (0,)), ((), ())), preferred_element_type=F32)


def nt(left, right):
    return lax.dot_general(left, right, (((1,), (1,)), ((), ())), preferred_element_type=F32)


def tn(left, right):
    return lax.dot_general(left, right, (((0,), (0,)), ((), ())), preferred_element_type=F32)


def layer_kernel(
    groups, lanes, across,
    moe_ref, cot_ref, route_ref, weight_ref, mean_ref, rstd_ref, conv_ref, gain_ref, shift_ref, taps_ref,
    gate_hbm, up_hbm, down_hbm, proj_hbm,
    gup_ref, gdown_ref, gstream_ref, gproj_ref, gconv_ref,
    gate_w, up_w, down_w, send, rows, work_a, work_b, work_c, hid, upg, gtg,
    part, half, summed, arrived, total, returned, chosen_back, gathered, mix, pieces,
    lines_s, normed_s, slope_s, stat_out, stat_in, ext,
    load_sem, dsp_s, dsp_r, dy_s, dy_r, dc_s, dc_r, sw_s, sw_r, cy_s, cy_r, csp_s, csp_r,
    az_s, az_r, ax_s, ax_r, ty_s, ty_r, tc_s, tc_r, p_s, p_r, py_s, py_r, pc_s, pc_r, st_s, st_r, halo_s, halo_r,
):
    group, lane = (lax.axis_index("sp"), lax.axis_index("tp"))
    chips = lanes // 2
    depth = groups // across
    chip, core = (lax.div(lane, 2), lax.rem(lane, 2))
    level, column = (lax.div(group, across), lax.rem(group, across))
    tokens, width = moe_ref.shape
    channels = width * lanes
    hidden_units = gate_w.shape[0]
    slots = groups * (rows.shape[1] // groups)
    cap = slots // groups
    chunks = ((0, groups // 2), (groups // 2, 3 * groups // 4), (3 * groups // 4, groups))
    proj_rows = proj_hbm.shape[0]
    lag_count = taps_ref.shape[0]
    partner = (group, flipped(lane, 1))
    mine = tile(lane, width)

    barrier = pltpu.get_barrier_semaphore()
    for step in range(1, groups):
        pl.semaphore_signal(barrier, inc=1, device_id=(flipped(group, step), lane), device_id_type=MESH)
    for step in range(1, lanes):
        pl.semaphore_signal(barrier, inc=1, device_id=(group, flipped(lane, step)), device_id_type=MESH)

    def remote(source, target, sends, recvs, device):
        return pltpu.make_async_remote_copy(
            src_ref=source, dst_ref=target, send_sem=sends, recv_sem=recvs,
            device_id=device, device_id_type=MESH,
        )

    loads = [
        pltpu.make_async_copy(proj_hbm, gathered.at[group, pl.ds(0, proj_rows)], load_sem.at[0]),
        pltpu.make_async_copy(gate_hbm.at[0], gate_w, load_sem.at[1]),
        pltpu.make_async_copy(up_hbm.at[0], up_w, load_sem.at[2]),
        pltpu.make_async_copy(down_hbm.at[0], down_w, load_sem.at[3]),
    ]
    for copy in loads:
        copy.start()

    lines_s[...] = jnp.zeros(lines_s.shape, F32)
    lines_s[0:2, 0:tokens] = (route_ref[...] ^ group).astype(F32)
    lines_s[2:3, 0:tokens] = mean_ref[...]
    lines_s[3:4, 0:tokens] = rstd_ref[...]
    named_line = (lines_s[0:1, 0:tokens], lines_s[1:2, 0:tokens])
    weight_line = (weight_ref[0:1, :], weight_ref[1:2, :])
    columns = lines_s[...].T
    named_col = (columns[0:tokens, 0:1], columns[0:tokens, 1:2])
    mean_col, rstd_col = (columns[0:tokens, 2:3], columns[0:tokens, 3:4])
    down_iota = lax.broadcasted_iota(jnp.int32, (tokens, tokens), 0)
    over_iota = lax.broadcasted_iota(jnp.int32, (tokens, tokens), 1)
    targets = []
    for choice in range(2):
        same = jnp.where(named_col[0] == named_line[choice], 1.0, 0.0) + jnp.where(
            named_col[1] == named_line[choice], 1.0, 0.0
        )
        rank = jnp.sum(jnp.where(down_iota < over_iota, same, 0.0), axis=0, keepdims=True)
        targets.append(named_line[choice] * float(cap) + rank)

    def fill(low, high):
        here = slice(low * cap, high * cap)
        count = (high - low) * cap
        place = lax.broadcasted_iota(jnp.int32, (count, tokens), 0).astype(F32) + float(low * cap)
        first, second = (place == targets[0], place == targets[1])
        slot_weight = jnp.sum(
            jnp.where(first, weight_line[0], 0.0) + jnp.where(second, weight_line[1], 0.0),
            axis=1, keepdims=True,
        )
        chosen = jnp.where(first | second, 1.0, 0.0).astype(BF)
        send[0, here, :] = nn(chosen, moe_ref[...]).astype(BF)
        send[1, here, :] = (slot_weight * nn(chosen, cot_ref[...])).astype(BF)

    fill(0, groups // 2)
    rows[0, 0:cap, mine] = send[0, 0:cap, :]
    rows[1, 0:cap, mine] = send[1, 0:cap, :]

    pl.semaphore_wait(barrier, groups + lanes - 2)

    def at_slot(step, lane_index):
        return rows.at[:, pl.ds(step * cap, cap), tile(lane_index, width)]

    outgoing = []

    def go(copy, alone=True):
        copy.start()
        if alone:
            outgoing.append(copy)
        return copy

    dispatched, crossed, shared = ({}, {}, {})

    def forward(step):
        for turn in range(1, chips):
            crossed[step, turn] = go(remote(
                at_slot(step, lane), at_slot(step, lane), dy_s.at[turn - 1], dy_r.at[step, turn - 1],
                (group, flipped(lane, 2 * turn)),
            ), alone=False)
        shared[step, 0] = go(remote(
            at_slot(step, lane), at_slot(step, lane), dc_s.at[0], dc_r.at[step, 0], partner
        ), alone=False)

    def relay(step):
        for turn in range(1, chips):
            crossed[step, turn].wait_recv()
            peer = flipped(lane, 2 * turn)
            shared[step, turn] = go(remote(
                at_slot(step, peer), at_slot(step, peer), dc_s.at[turn], dc_r.at[step, turn], partner
            ), alone=False)

    def dispatch(step):
        dispatched[step] = go(remote(
            send.at[:, pl.ds(step * cap, cap)], at_slot(step, lane),
            dsp_s.at[0], dsp_r.at[step], (flipped(group, step), lane),
        ), alone=False)

    forward(0)
    for step in range(1, groups // 2):
        dispatch(step)
    fill(groups // 2, groups)
    for step in range(groups // 2, 3 * groups // 4):
        dispatch(step)

    bounds = ((0, proj_rows), (proj_rows, tokens))

    def block(owner_level, owner_column, kind):
        return gathered.at[owner_level * across + owner_column, pl.ds(bounds[kind][0], bounds[kind][1])]

    def along(kind, way, hop):
        sign = 1 - 2 * way
        source_level = level - sign * hop
        here = block(source_level, column, kind)
        return remote(
            here, here, az_s.at[kind, way, hop], az_r.at[kind, way, hop],
            ((level + sign) * across + column, lane),
        )

    def along_valid(way, hop):
        if way == 0:
            return (level - hop >= 0) & (level + 1 < depth)
        return (level + hop < depth) & (level - 1 >= 0)

    def arrives_valid(way, hop):
        if way == 0:
            return level - 1 - hop >= 0
        return level + 1 + hop < depth

    def sideways(kind, event, owner_level):
        copies = []
        for turn in range(1, across):
            here = block(owner_level, column, kind)
            copies.append(remote(
                here, here, ax_s.at[kind, event, turn - 1], ax_r.at[kind, event, turn - 1],
                (level * across + flipped(column, turn), lane),
            ))
        return copies

    def over_middle(way, source_level, wanted):
        edge_level = depth // 2 - 1 + way
        return (source_level == edge_level) if wanted else (source_level != edge_level)

    def gather_along(kind, middle):
        for way in range(2):
            @pl.when(along_valid(way, 0) & over_middle(way, level, middle))
            def _():
                along(kind, way, 0).start()

    def gather_sideways(kind):
        for copy in sideways(kind, 0, level):
            copy.start()

    def gather_hop(kind, hop, middle=None):
        for way in range(2):
            sign = 1 - 2 * way
            due = arrives_valid(way, hop)
            if middle is not None:
                due = due & over_middle(way, level - sign, middle)

            @pl.when(due)
            def _():
                along(kind, way, hop).wait_recv()
                if hop + 1 < depth - 1:
                    @pl.when(along_valid(way, hop + 1))
                    def _():
                        along(kind, way, hop + 1).start()
                for copy in sideways(kind, 1 + 2 * hop + way, level - sign * (hop + 1)):
                    copy.start()

    def gather_rest(kind):
        for copy in sideways(kind, 0, level):
            copy.wait()
        for hop in range(depth - 1):
            for way in range(2):
                sign = 1 - 2 * way

                @pl.when(along_valid(way, hop))
                def _():
                    along(kind, way, hop).wait_send()

                @pl.when(arrives_valid(way, hop))
                def _():
                    for copy in sideways(kind, 1 + 2 * hop + way, level - sign * (hop + 1)):
                        copy.wait()


    normed = (conv_ref[...].astype(F32) - mean_col) * rstd_col
    pre_act = normed * gain_ref[...] + shift_ref[...]
    act_sigmoid = jax.nn.sigmoid(pre_act)
    gathered[group, proj_rows : proj_rows + tokens, :] = (pre_act * act_sigmoid).astype(BF)
    normed_s[...] = normed
    slope_s[...] = act_sigmoid * (1.0 + pre_act * (1.0 - act_sigmoid)) * gain_ref[...]
    back_place = lax.broadcasted_iota(jnp.int32, (tokens, slots), 1).astype(F32)
    back = None
    for choice in range(2):
        same = jnp.where(named_line[0] == named_col[choice], 1.0, 0.0) + jnp.where(
            named_line[1] == named_col[choice], 1.0, 0.0
        )
        rank = jnp.sum(jnp.where(over_iota < down_iota, same, 0.0), axis=1, keepdims=True)
        match = back_place == named_col[choice] * float(cap) + rank
        back = match if back is None else back | match
    chosen_back[...] = jnp.where(back, 1.0, 0.0).astype(BF)

    def of_chunk(part_index):
        return slice(chunks[part_index][0] * cap, chunks[part_index][1] * cap)

    def activate(part_index):
        here = of_chunk(part_index)
        step_rows = 64
        count = here.stop - here.start

        def body(index, carry):
            there = tile(index, step_rows)
            gate_pre, up_pre, hidden_grad = (
                work_a[there, 0:count], work_b[there, 0:count], work_c[there, 0:count]
            )
            gate_sigmoid = jax.nn.sigmoid(gate_pre)
            gate_active = gate_pre * gate_sigmoid
            hid[there, here] = (gate_active * up_pre).astype(BF)
            upg[there, here] = (hidden_grad * gate_active).astype(BF)
            gtg[there, here] = (
                hidden_grad * up_pre * (gate_sigmoid * (1.0 + gate_pre * (1.0 - gate_sigmoid)))
            ).astype(BF)
            return carry

        lax.fori_loop(0, hidden_units // step_rows, body, 0)

    def partial_columns(part_index, lane_index):
        here = of_chunk(part_index)
        there = tile(lane_index, width)
        value = tn(gtg[:, here], gate_w[:, there]) + tn(upg[:, here], up_w[:, there])
        part[here, there] = value.astype(BF)

    swaps, homeward, back_across = ({}, {}, {})

    def swap(part_index, turn):
        away = flipped(lane, 2 * turn + 1)
        here = pl.ds(chunks[part_index][0] * cap, (chunks[part_index][1] - chunks[part_index][0]) * cap)
        swaps[part_index, turn] = go(remote(
            part.at[here, tile(away, width)], half.at[turn, here],
            sw_s.at[part_index, turn], sw_r.at[part_index, turn], partner,
        ))

    def partials(part_index, between):
        for turn in [*range(1, chips), 0]:
            partial_columns(part_index, flipped(lane, 2 * turn + 1))
            swap(part_index, turn)
            partial_columns(part_index, flipped(lane, 2 * turn))
            if turn == 1:
                between()

    def chip_sums(part_index):
        for turn in range(1, chips):
            away = flipped(lane, 2 * turn)
            swaps[part_index, turn].wait_recv()
            for step in range(*chunks[part_index]):
                here = slice(step * cap, (step + 1) * cap)
                summed[turn - 1, here, :] = (
                    part[here, tile(away, width)].astype(F32) + half[turn, here, :].astype(F32)
                ).astype(BF)
                back_across[step, turn] = go(remote(
                    summed.at[turn - 1, pl.ds(step * cap, cap)], arrived.at[turn - 1, pl.ds(step * cap, cap)],
                    cy_s.at[turn - 1], cy_r.at[step, turn - 1], (group, away),
                ), alone=False)

    def send_home(part_index):
        swaps[part_index, 0].wait_recv()
        for step in range(*chunks[part_index]):
            here = slice(step * cap, (step + 1) * cap)
            value = part[here, mine].astype(F32) + half[0, here, :].astype(F32)
            for turn in range(1, chips):
                back_across[step, turn].wait_recv()
                value = value + arrived[turn - 1, here, :].astype(F32)
            if step:
                total[here, :] = value.astype(BF)
                homeward[step] = go(remote(
                    total.at[pl.ds(step * cap, cap)], returned.at[pl.ds(step * cap, cap)],
                    csp_s.at[0], csp_r.at[step], (flipped(group, step), lane),
                ), alone=False)
            else:
                returned[here, :] = value.astype(BF)

    def first_matmuls(part_index, between):
        here = of_chunk(part_index)
        count = here.stop - here.start
        for work, weight, source in ((work_a, gate_w, 0), (work_b, up_w, 0), (work_c, down_w, 1)):
            work[:, 0:count] = nt(weight[...], rows[source, here, :])
            between.pop(0)()

    def advance(low, high):
        for step in range(low, high):
            dispatched[step].wait_recv()
            forward(step)
            if step % 2:
                dispatch(3 * groups // 4 + step // 2)
            relay(step - 1)

    def pass_on(low, high):
        for step in range(low, high):
            dispatched[step].wait_recv()
            forward(step)

    def relays(low, high):
        for step in range(low, high):
            relay(step)

    def complete(part_index):
        for step in range(*chunks[part_index]):
            for turn in range(chips):
                shared[step, turn].wait_recv()

    def nothing():
        return None

    first_edge, second_edge = (chunks[0][1], chunks[1][1])
    first_half, second_half = ((first_edge + second_edge) // 2, (second_edge + groups) // 2)
    advance(1, first_edge)
    loads[0].wait()
    for kind in range(2):
        gather_along(kind, False)
        gather_sideways(kind)
    relays(first_edge - 1, first_edge)
    complete(0)
    pass_on(first_edge, first_half)
    for copy in loads[1:]:
        copy.wait()
    gather_along(0, True)
    first_matmuls(0, [lambda: pass_on(first_half, second_edge), nothing, lambda: pass_on(second_edge, second_half)])
    activate(0)
    relays(first_edge, first_half)

    def rest_of_dispatch():
        pass_on(second_half, groups)
        relays(first_half, second_edge)

    partials(0, rest_of_dispatch)
    relays(second_edge, second_half)
    chip_sums(0)
    gather_hop(0, 0, False)
    gather_along(1, True)
    gather_hop(1, 0, False)
    complete(1)
    first_matmuls(1, [nothing, nothing, nothing])
    relays(second_half, groups)
    gather_hop(0, 0, True)
    activate(1)
    partials(1, nothing)
    chip_sums(1)
    complete(2)
    first_matmuls(2, [nothing, nothing, nothing])
    gather_hop(0, 1)
    send_home(0)
    activate(2)
    send_home(1)
    partials(2, nothing)
    chip_sums(2)
    send_home(2)
    gather_hop(1, 0, True)

    span = min(channels, 512)

    def down_tile(index, carry):
        there = tile(index, span)
        gdown_ref[0, :, there] = nn(hid[...], rows[1, :, there]).astype(BF)
        return carry

    def up_tile(index, carry):
        there = tile(index, span)
        gup_ref[0, :, there] = nn(upg[...], rows[0, :, there]).astype(BF)
        return carry

    lax.fori_loop(0, channels // span, down_tile, 0)
    lax.fori_loop(0, channels // span, up_tile, 0)
    for hop in range(2, depth - 1):
        gather_hop(0, hop)
    gather_hop(1, 1, True)

    for step in range(1, groups):
        homeward[step].wait_recv()
    picked = nn(chosen_back[...], returned[...])
    own_stream = (cot_ref[...].astype(F32) + picked).astype(BF)
    gstream_ref[...] = own_stream
    mix[:, mine] = own_stream
    tp_across = {}
    for turn in range(1, chips):
        tp_across[turn] = go(remote(
            mix.at[:, mine], mix.at[:, mine], ty_s.at[turn], ty_r.at[turn], (group, flipped(lane, 2 * turn))
        ))
    tp_shared = {0: go(remote(mix.at[:, mine], mix.at[:, mine], tc_s.at[0], tc_r.at[0], partner))}
    for turn in range(1, chips):
        tp_across[turn].wait_recv()
        theirs = tile(flipped(lane, 2 * turn), width)
        tp_shared[turn] = go(remote(
            mix.at[:, theirs], mix.at[:, theirs], tc_s.at[turn], tc_r.at[turn], partner
        ))
    gather_hop(1, 1, False)
    for turn in range(chips):
        tp_shared[turn].wait_recv()

    share = channels // groups
    piece_width = pieces.shape[3]
    quarter = tokens // 4
    place_of_four = lax.rem(lane, 4)

    def piece_of(owner):
        if share == piece_width:
            return tile(owner, share)
        return tile(lax.div(owner * share, piece_width), piece_width)

    travelling, piece_across, piece_shared = ({}, {}, {})
    for step in range(1, groups):
        owner = flipped(group, step)
        travelling[step] = go(remote(
            mix.at[tile(place_of_four, quarter), piece_of(owner)], pieces.at[step, place_of_four],
            p_s.at[0], p_r.at[step], (owner, lane),
        ), alone=False)

    def piece_forward(step):
        travelling[step].wait_recv()
        here = pieces.at[step, place_of_four]
        piece_across[step] = go(remote(
            here, here, py_s.at[0], py_r.at[step], (group, flipped(lane, 2))
        ), alone=False)
        piece_shared[step, 0] = go(remote(here, here, pc_s.at[0], pc_r.at[step, 0], partner), alone=False)

    def piece_relay(step):
        piece_across[step].wait_recv()
        here = pieces.at[step, flipped(place_of_four, 2)]
        piece_shared[step, 1] = go(remote(here, here, pc_s.at[1], pc_r.at[step, 1], partner), alone=False)

    gather_rest(0)
    whole_proj = gathered[:, 0:proj_rows, :].reshape(groups * proj_rows, width)
    normed_grad = nn(mix[...], whole_proj) * slope_s[...]
    weighted = normed_grad * normed_s[...]
    ones = jnp.ones((16, width), BF)

    def line_sum(value):
        high = value.astype(BF)
        low = (value - high.astype(F32)).astype(BF)
        return nt(ones, high) + nt(ones, low)

    line = lax.broadcasted_iota(jnp.int32, (16, tokens), 0)
    own_stat = jnp.where(line == 0, line_sum(normed_grad), line_sum(weighted))
    stat_out[...] = own_stat
    stats = []
    for step in range(1, lanes):
        stats.append(go(remote(
            stat_out, stat_in.at[step], st_s.at[step], st_r.at[step], (group, flipped(lane, step))
        )))
    all_stat = own_stat
    for step in range(1, lanes):
        stats[step - 1].wait_recv()
        all_stat = all_stat + stat_in[step]
    all_stat = all_stat * (1.0 / channels)
    high = all_stat.astype(BF)
    middle = (all_stat - high.astype(F32)).astype(BF)
    low = (all_stat - high.astype(F32) - middle.astype(F32)).astype(BF)
    pick = lax.broadcasted_iota(jnp.int32, (16, width), 0)

    def spread_line(number):
        chooser = jnp.where(pick == number, 1.0, 0.0).astype(BF)
        return tn(high, chooser) + tn(middle, chooser) + tn(low, chooser)

    first_line, second_line = (spread_line(0), spread_line(1))
    rim = ext.shape[0] - tokens

    def halo():
        return remote(
            ext.at[pl.ds(0, rim)], ext.at[pl.ds(tokens, rim)], halo_s, halo_r, (group - 1, lane)
        )

    def conv_gradient(here):
        ext[here, :] = rstd_col[here] * (
            normed_grad[here] - first_line[here] - normed_s[here, :] * second_line[here]
        )

    conv_gradient(slice(0, rim))

    @pl.when(group > 0)
    def _():
        halo().start()

    conv_gradient(slice(rim, tokens))
    for hop in range(2, depth - 1):
        gather_hop(1, hop)
    for step in range(1, groups):
        piece_forward(step)

    @pl.when(group < groups - 1)
    def _():
        halo().wait_recv()

    @pl.when(group == groups - 1)
    def _():
        ext[tokens : tokens + rim, :] = jnp.zeros((rim, width), F32)

    def conv_tile(index, carry):
        there = tile(index, 128)
        chunk = 64
        for start in range(0, tokens, chunk):
            value = jnp.zeros((chunk, 128), F32)
            for lag in range(lag_count):
                value = value + taps_ref[lag : lag + 1, there] * ext[start + lag : start + lag + chunk, there]
            gconv_ref[start : start + chunk, there] = value.astype(BF)
        return carry

    lax.fori_loop(0, width // 128, conv_tile, 0)

    def piece_value(value):
        if share == piece_width:
            return value
        per = piece_width // share
        which = lax.rem(group, per)
        result = value[:, 0:share]
        for index in range(1, per):
            result = jnp.where(which == index, value[:, index * share : (index + 1) * share], result)
        return result

    for step in range(1, groups):
        piece_relay(step)
    gather_rest(1)
    gproj = tn(piece_value(mix[:, piece_of(group)]), gathered[group, proj_rows : proj_rows + tokens, :])
    for step in range(1, groups):
        for turn in range(2):
            piece_shared[step, turn].wait_recv()
        owner = flipped(group, step)
        gproj = gproj + tn(piece_value(pieces[step].reshape(tokens, piece_width)), gathered[owner, proj_rows : proj_rows + tokens, :])
    gproj_ref[...] = gproj

    @pl.when(group > 0)
    def _():
        halo().wait_send()

    for copy in outgoing:
        copy.wait_send()

    def all_sent(source, sends, recvs):
        remote(source, source, sends, recvs, partner).wait_send()

    later = pl.ds(cap, slots - cap)
    all_sent(send.at[:, later], dsp_s.at[0], dsp_r.at[0])
    all_sent(total.at[later], csp_s.at[0], csp_r.at[0])
    for turn in range(chips):
        all_sent(send, dc_s.at[turn], dc_r.at[0, turn])
        if turn:
            all_sent(send, dy_s.at[turn - 1], dy_r.at[0, turn - 1])
            all_sent(total, cy_s.at[turn - 1], cy_r.at[0, turn - 1])
    every_piece = pieces.at[pl.ds(1, groups - 1), 0]
    for sends, recvs in ((p_s.at[0], p_r.at[0]), (py_s.at[0], py_r.at[0]), (pc_s.at[0], pc_r.at[0, 0]), (pc_s.at[1], pc_r.at[0, 1])):
        all_sent(every_piece, sends, recvs)


def on_device(
    moe_in, cotangent, routes, route_weight, w_gate, w_up, w_down,
    conv_pre, norm_mean, norm_rstd, ln_gain, ln_shift, taps, w_proj,
):
    groups, lanes = (lax.axis_size("sp"), lax.axis_size("tp"))
    chips = lanes // 2
    across = 1 << (groups.bit_length() // 2 - 1)
    depth = groups // across
    tokens, width = moe_in.shape
    channels = width * lanes
    hidden_units = w_gate.shape[1]
    cap = (5 * tokens // (2 * groups) + 15) // 16 * 16
    slots = groups * cap
    proj_rows = w_proj.shape[0]
    share = channels // groups
    piece_width = max(share, 128)
    rim = (taps.shape[0] - 1 + 7) // 8 * 8
    vmem_limit = 48 * 1024 * 1024
    dma = pltpu.SemaphoreType.DMA
    vmem = pltpu.VMEM
    others = max(1, chips - 1)
    inside = pl.BlockSpec(memory_space=pltpu.VMEM)
    outside = pl.BlockSpec(memory_space=pl.ANY)
    results = pl.pallas_call(
        functools.partial(layer_kernel, groups, lanes, across),
        out_shape=(
            vmem(w_up.shape, BF),
            vmem(w_down.shape, BF),
            vmem((tokens, width), BF),
            vmem((proj_rows, width), F32),
            vmem((tokens, width), BF),
        ),
        in_specs=[inside] * 10 + [outside] * 4,
        out_specs=(inside,) * 5,
        scratch_shapes=[
            vmem((hidden_units, channels), BF), vmem((hidden_units, channels), BF), vmem((hidden_units, channels), BF),
            vmem((2, slots, width), BF), vmem((2, slots, channels), BF),
            vmem((hidden_units, slots // 2), F32), vmem((hidden_units, slots // 2), F32), vmem((hidden_units, slots // 2), F32),
            vmem((hidden_units, slots), BF), vmem((hidden_units, slots), BF), vmem((hidden_units, slots), BF),
            vmem((slots, channels), BF), vmem((chips, slots, width), BF),
            vmem((others, slots, width), BF), vmem((others, slots, width), BF),
            vmem((slots, width), BF), vmem((slots, width), BF), vmem((tokens, slots), BF),
            vmem((groups, proj_rows + tokens, width), BF), vmem((tokens, channels), BF),
            vmem((groups, 4, tokens // 4, piece_width), BF),
            vmem((128, (tokens + 127) // 128 * 128), F32), vmem((tokens, width), F32), vmem((tokens, width), F32),
            vmem((16, tokens), F32), vmem((lanes, 16, tokens), F32), vmem((tokens + rim, width), F32),
            dma((4,)), dma((1,)), dma((groups,)),
            dma((others,)), dma((groups, others)), dma((chips,)), dma((groups, chips)),
            dma((3, chips)), dma((3, chips)), dma((others,)), dma((groups, others)),
            dma((1,)), dma((groups,)),
            dma((2, 2, depth - 1)), dma((2, 2, depth - 1)),
            dma((2, 2 * depth - 1, across - 1)), dma((2, 2 * depth - 1, across - 1)),
            dma((chips,)), dma((chips,)), dma((chips,)), dma((chips,)),
            dma((1,)), dma((groups,)), dma((1,)), dma((groups,)), dma((2,)), dma((groups, 2)),
            dma((lanes,)), dma((lanes,)), dma, dma,
        ],
        compiler_params=pltpu.CompilerParams(
            collective_id=1, has_side_effects=True, vmem_limit_bytes=vmem_limit
        ),
    )(
        moe_in, cotangent, routes.T, route_weight.T, norm_mean[None, :], norm_rstd[None, :], conv_pre, ln_gain[None, :], ln_shift[None, :], taps,
        w_gate, w_up, w_down, w_proj,
    )
    return pl.pallas_call(
        write_kernel,
        out_shape=tuple(jax.ShapeDtypeStruct(result.shape, result.dtype) for result in results),
        in_specs=[inside] * 5,
        out_specs=(outside,) * 5,
        scratch_shapes=[dma((5,))],
        compiler_params=pltpu.CompilerParams(vmem_limit_bytes=16 * 1024 * 1024),
    )(*results)


def write_kernel(*refs):
    copies = [pltpu.make_async_copy(refs[index], refs[5 + index], refs[10].at[index]) for index in range(5)]
    for copy in copies:
        copy.start()
    for copy in copies:
        copy.wait()


def solution(mesh):
    placed = (
        P("sp", "tp"), P("sp", "tp"), P("sp", None), P("sp", None),
        P("sp", "tp", None), P("sp", "tp", None), P("sp", "tp", None),
        P("sp", "tp"), P("sp"), P("sp"), P("tp"), P("tp"), P(None, "tp"), P("sp", "tp"),
    )
    return jax.shard_map(
        on_device,
        mesh=mesh,
        in_specs=placed,
        out_specs=(
            P("sp", "tp", None), P("sp", "tp", None), P("sp", "tp"), P("sp", "tp"), P("sp", "tp"),
        ),
        check_vma=False,
    )
```
